32 devices in a mesh: kv: 8 (over z, y), tp: 4 (over x, core).
Axes of the slice: x: 2, y: 2, z: 4, core: 2. Of those that a mesh axis runs over, the one named last changes fastest.
Arguments:
- queries: bfloat16 [1024, 1024], P('kv', 'tp'), may hold values from -6 to 6
- keys: bfloat16 [1024, 512], P('kv', 'tp'), may hold values from -6 to 6
- values: bfloat16 [1024, 512], P('kv', 'tp'), may hold values from -6 to 6
- hidden: bfloat16 [1024, 2048], P('kv'), may hold values from -6 to 6
- log_sums: float32 [2, 1024, 16], P(None, 'kv', 'tp'), may hold values from -1 to 12
- gates: float32 [2, 1024, 16], P(None, 'kv', 'tp'), may hold values from 0.1 to 0.9
- branch_out: bfloat16 [2, 1024, 1024], P(None, 'kv', 'tp'), may hold values from -6 to 6
- cotangent: bfloat16 [1024, 1024], P('kv', 'tp'), may hold values from -6 to 6
- chosen: int32 [8, 8, 48], P(None, 'tp'), may hold values from -1 to 31, as said below
Outputs:
- grad_queries: float32 [1024, 1024], P('kv', 'tp')
- grad_keys: float32 [1024, 512], P('kv', 'tp')
- grad_values: float32 [1024, 512], P('kv', 'tp')
- grad_weight: float32 [2048, 1024], P('kv', 'tp')
The draws below stay inside these ranges and needn't reach their ends.
Inputs may be any that keep to these rules, and one draw needn't show every extreme that they name: `chosen`: each list holds global block numbers or -1. All live entries of one list name blocks of distinct owners, owner = entry // 4, none later than the list's range; list d holds min(48, d + 1) live entries, and they come first.
All inputs are finite; a program needn't handle non-finite values.
Results may differ from the reference program's by a relative error of at most 0.0055.
Values may be sent and summed in bfloat16 or wider, within the bound.
A program may use at most 64 MiB of HBM per device.

```python
import jax
import jax.numpy as jnp
from jax import lax

D = 2048
HQ = 16
KVG = 8
DH = 64
BLK = 32
TOPN = 12
SUB = 4
CMP = 32
TOK_DEV = 128
TOKENS = 1024


def draw_log_sums(key, part):
    position = jnp.arange(TOKENS, dtype=jnp.int32)
    device = position // TOK_DEV
    sub_index = position % TOK_DEV // (TOK_DEV // SUB)
    summary_seen = jnp.maximum((position + 1) // CMP, 1).astype(jnp.float32)
    live_here = jnp.clip(jnp.minimum(SUB * TOPN, device + 1) - sub_index * TOPN, 1, TOPN)
    block_seen = (live_here * BLK).astype(jnp.float32)
    base = jnp.stack([jnp.log(summary_seen), jnp.log(block_seen) + 0.5])[:, :, None]
    noise = jnp.clip(jax.random.normal(key, (2, TOKENS, HQ), jnp.float32) * 0.3, -0.9, 0.9)
    return base + noise


def draw_chosen(key, part):
    blocks_all = TOKENS // TOK_DEV
    per_block = TOK_DEV // BLK
    nsel = SUB * TOPN
    taken_count = min(nsel, blocks_all)
    first_key = jax.random.fold_in(key, 11)
    second_key = jax.random.fold_in(key, 23)
    device = jnp.arange(blocks_all, dtype=jnp.int32)[:, None, None]
    owner = jnp.arange(blocks_all, dtype=jnp.int32)[None, None, :]
    random_part = jax.random.randint(first_key, (blocks_all, KVG, blocks_all), 0, 1000) * blocks_all + owner
    forced = (owner == device) | (owner == device - 1) | (owner == device - blocks_all // 2) | (owner == 0)
    score = jnp.where(owner <= device, random_part + forced.astype(jnp.int32) * (2000 * blocks_all), -1)
    top_score, picks = lax.top_k(score, taken_count)
    inner = jax.random.randint(second_key, (blocks_all, KVG, taken_count), 0, per_block - 1)
    far_pick = (picks == device - blocks_all // 2) & (device >= blocks_all // 2)
    inner = jnp.where(far_pick, per_block - 1, inner)
    listing = jnp.where(top_score >= 0, picks * per_block + inner, -1).astype(jnp.int32)
    if nsel > taken_count:
        filler = jnp.full((blocks_all, KVG, nsel - taken_count), -1, jnp.int32)
        listing = jnp.concatenate([listing, filler], -1)
    return listing


def block_levels(own_key, dims, pieces, low, high):
    def one(dim, shards_of):
        steps = jax.random.uniform(jax.random.fold_in(jax.random.fold_in(own_key, 6), dim), (shards_of,), jnp.float32, low / len(pieces), high / len(pieces))
        return jnp.repeat(jnp.exp(steps), dims[dim] // shards_of).reshape((-1,) + (1,) * (len(dims) - dim - 1))

    factor_of = one(*pieces[0])
    for cut in pieces[1:]:
        factor_of = factor_of * one(*cut)
    return factor_of


def gaussian(key, dims, width, bound, pieces=(), kind=jnp.bfloat16):
    drawn = jax.random.normal(key, dims, jnp.float32) * width
    if len(pieces) > 0:
        drawn = block_levels(key, dims, pieces, -0.22, 0.18) * drawn
    return jnp.clip(drawn, min=-bound, max=bound).astype(kind)


def setup_inputs(seed: int = 0) -> dict:
    streams_of = jax.random.split(jax.random.key(seed), 10)
    queries = gaussian(streams_of[0], (TOKENS, HQ * DH), 1.0, 6.0, ((0, 8), (1, 4)))
    keys = gaussian(streams_of[1], (TOKENS, KVG * DH), 1.0, 6.0, ((0, 8), (1, 4)))
    values = gaussian(streams_of[2], (TOKENS, KVG * DH), 1.0, 6.0, ((0, 8), (1, 4)))
    hidden = gaussian(streams_of[3], (TOKENS, D), 1.0, 6.0, ((0, 8),))
    log_sums = draw_log_sums(jax.random.fold_in(streams_of[9], 71), 0)
    gates = jnp.clip(0.1 + 0.79999997 * jax.random.uniform(streams_of[5], (2, TOKENS, HQ), jnp.float32) ** block_levels(streams_of[5], (2, TOKENS, HQ), ((1, 8), (2, 4)), -0.2, 0.2), 0.1, 0.9)
    branch_out = gaussian(streams_of[6], (2, TOKENS, HQ * DH), 1.0, 6.0, ((1, 8), (2, 4)))
    cotangent = gaussian(streams_of[7], (TOKENS, HQ * DH), 1.0, 6.0, ((0, 8), (1, 4)))
    chosen = draw_chosen(jax.random.fold_in(streams_of[9], 71), 0)
    return {"queries": queries, "keys": keys, "values": values, "hidden": hidden, "log_sums": log_sums, "gates": gates, "branch_out": branch_out, "cotangent": cotangent, "chosen": chosen}


def branch_grads(query_rows, key_rows, value_rows, seen, log_rows, delta_rows, cot_rows, scale):
    wide = jnp.float32
    scores = jnp.einsum('tgre,gme->grtm', query_rows.astype(wide), key_rows.astype(wide)) * scale
    log_here = jnp.transpose(log_rows, (1, 2, 0))[..., None]
    delta_here = jnp.transpose(delta_rows, (1, 2, 0))[..., None]
    probs = jnp.where(seen[:, None], jnp.exp(scores - log_here), 0.0)
    probs_low = lax.optimization_barrier(probs.astype(jnp.bfloat16)).astype(wide)
    value_grad = jnp.einsum('grtm,tgre->gme', probs_low, cot_rows.astype(wide))
    prob_grad = jnp.einsum('tgre,gme->grtm', cot_rows.astype(wide), value_rows.astype(wide))
    score_grad = probs * (prob_grad - delta_here)
    score_low = lax.optimization_barrier(score_grad.astype(jnp.bfloat16)).astype(wide)
    query_grad = jnp.einsum('grtm,gme->tgre', score_low, key_rows.astype(wide)) * scale
    key_grad = jnp.einsum('grtm,tgre->gme', score_low, query_rows.astype(wide)) * scale
    return query_grad, key_grad, value_grad


def reference(queries, keys, values, hidden, log_sums, gates, branch_out, cotangent, chosen):
    wide = jnp.float32
    group_heads = HQ // KVG
    nsel = SUB * TOPN
    qrows = TOK_DEV // SUB
    scale = DH ** -0.5
    summary_count = TOKENS // CMP
    grads_each = jax.vmap(branch_grads, in_axes=(0, 0, 0, 0, 0, 0, 0, None))
    query_all = queries.reshape(TOKENS, KVG, group_heads, DH)
    gated = gates[..., None] * cotangent.reshape(TOKENS, HQ, DH).astype(wide)[None]
    delta_all = jnp.sum(gated * branch_out.reshape(2, TOKENS, HQ, DH).astype(wide), -1)
    delta_all = delta_all.reshape(2, TOKENS, KVG, group_heads)
    gated_low = gated.astype(jnp.bfloat16).reshape(2, TOKENS, KVG, group_heads, DH)
    log_all = log_sums.reshape(2, TOKENS, KVG, group_heads)
    sum_keys = jnp.mean(keys.reshape(summary_count, CMP, KVG, DH).astype(wide), 1).astype(jnp.bfloat16)
    sum_values = jnp.mean(values.reshape(summary_count, CMP, KVG, DH).astype(wide), 1).astype(jnp.bfloat16)
    sum_keys = jnp.transpose(sum_keys, (1, 0, 2))
    sum_values = jnp.transpose(sum_values, (1, 0, 2))
    key_blocks = keys.reshape(TOKENS // BLK, BLK, KVG, DH)
    value_blocks = values.reshape(TOKENS // BLK, BLK, KVG, DH)
    group_index = jnp.arange(KVG, dtype=jnp.int32)[:, None]
    summary_end = jnp.arange(summary_count, dtype=jnp.int32) * CMP + CMP - 1

    def by_sub(array):
        rest = array.shape[3:]
        moved = array.reshape((KVG, SUB, TOPN * BLK) + rest)
        return jnp.swapaxes(moved, 0, 1)

    def step(carry, index):
        sel_keys, sel_values, summ_keys, summ_values = carry
        start = index * TOK_DEV
        query_here = lax.dynamic_slice_in_dim(query_all, start, TOK_DEV, 0)
        cot_here = lax.dynamic_slice_in_dim(gated_low, start, TOK_DEV, 1)
        log_here = lax.dynamic_slice_in_dim(log_all, start, TOK_DEV, 1)
        delta_here = lax.dynamic_slice_in_dim(delta_all, start, TOK_DEV, 1)
        position = start + jnp.arange(TOK_DEV, dtype=jnp.int32)
        summary_seen = (summary_end[None, :] <= position[:, None])[None]
        query_sum, key_sum, value_sum = branch_grads(query_here, sum_keys, sum_values, summary_seen,
                                                     log_here[0], delta_here[0], cot_here[0], scale)
        listing = lax.dynamic_index_in_dim(chosen, index, 0, keepdims=False)
        live = listing >= 0
        safe = jnp.maximum(listing, 0)
        picked_keys = by_sub(key_blocks[safe, :, group_index, :])
        picked_values = by_sub(value_blocks[safe, :, group_index, :])
        key_position = by_sub(safe[..., None] * BLK + jnp.arange(BLK, dtype=jnp.int32))
        live_rows = by_sub(jnp.broadcast_to(live[..., None], (KVG, nsel, BLK)))
        sub_position = position.reshape(SUB, qrows)
        block_seen = live_rows[:, :, None, :] & (key_position[:, :, None, :] <= sub_position[:, None, :, None])
        query_sel, key_sel, value_sel = grads_each(
            query_here.reshape(SUB, qrows, KVG, group_heads, DH), picked_keys, picked_values, block_seen,
            log_here[1].reshape(SUB, qrows, KVG, group_heads), delta_here[1].reshape(SUB, qrows, KVG, group_heads),
            cot_here[1].reshape(SUB, qrows, KVG, group_heads, DH), scale)
        query_sel = query_sel.reshape(TOK_DEV, KVG, group_heads, DH)
        key_sel = jnp.swapaxes(key_sel, 0, 1).reshape(KVG, nsel, BLK, DH)
        value_sel = jnp.swapaxes(value_sel, 0, 1).reshape(KVG, nsel, BLK, DH)
        weight_live = live[..., None, None].astype(wide)
        sel_keys = sel_keys.at[safe, :, group_index, :].add(key_sel * weight_live)
        sel_values = sel_values.at[safe, :, group_index, :].add(value_sel * weight_live)
        return (sel_keys, sel_values, summ_keys + key_sum, summ_values + value_sum), query_sum + query_sel

    start_state = (jnp.zeros((TOKENS // BLK, BLK, KVG, DH), wide), jnp.zeros((TOKENS // BLK, BLK, KVG, DH), wide),
                   jnp.zeros((KVG, summary_count, DH), wide), jnp.zeros((KVG, summary_count, DH), wide))
    final_state, query_blocks = lax.scan(step, start_state, jnp.arange(TOKENS // TOK_DEV, dtype=jnp.int32))
    sel_keys, sel_values, summ_keys, summ_values = final_state
    grad_queries = query_blocks.reshape(TOKENS, HQ * DH)
    grad_keys = sel_keys.reshape(TOKENS, KVG, DH) + jnp.repeat(jnp.transpose(summ_keys, (1, 0, 2)), CMP, axis=0) / CMP
    grad_values = sel_values.reshape(TOKENS, KVG, DH) + jnp.repeat(jnp.transpose(summ_values, (1, 0, 2)), CMP, axis=0) / CMP
    grad_weight = jnp.dot(hidden.T, grad_queries.astype(jnp.bfloat16), preferred_element_type=jnp.float32)
    return (grad_queries, grad_keys.reshape(TOKENS, KVG * DH), grad_values.reshape(TOKENS, KVG * DH), grad_weight)
```

```python
import functools

import jax
import jax.numpy as jnp
from jax import lax
from jax.experimental import pallas as pl
from jax.experimental.pallas import tpu as pltpu
from jax.sharding import PartitionSpec as P

DH = 64
BLK = 32
TOPN = 12
SUB = 4
CMP = 32


def branch_grads(query_rows, key_rows, value_rows, seen, log_rows, delta_rows, cot_rows, scale):
    wide = jnp.float32
    scores = jnp.einsum("tgre,gme->grtm", query_rows, key_rows, preferred_element_type=wide) * scale
    log_here = jnp.transpose(log_rows, (1, 2, 0))[..., None]
    delta_here = jnp.transpose(delta_rows, (1, 2, 0))[..., None]
    probs = jnp.where(seen[:, None], jnp.exp(scores - log_here), 0.0)
    probs_low = probs.astype(jnp.bfloat16)
    value_grad = jnp.einsum("grtm,tgre->gme", probs_low, cot_rows, preferred_element_type=wide)
    prob_grad = jnp.einsum("tgre,gme->grtm", cot_rows, value_rows, preferred_element_type=wide)
    score_low = (probs * (prob_grad - delta_here)).astype(jnp.bfloat16)
    query_grad = (
        jnp.einsum("grtm,gme->tgre", score_low, key_rows, preferred_element_type=wide) * scale
    )
    key_grad = (
        jnp.einsum("grtm,tgre->gme", score_low, query_rows, preferred_element_type=wide) * scale
    )
    return (query_grad, key_grad, value_grad)


def shards(queries, keys, values, hidden, log_sums, gates, branch_out, cotangent, chosen):
    wide = jnp.float32
    rows_here = queries.shape[0]
    heads = queries.shape[1] // DH
    groups = keys.shape[1] // DH
    group_heads = heads // groups
    per_block = rows_here // BLK
    per_summary = rows_here // CMP
    blocks_all = chosen.shape[0]
    nsel = chosen.shape[2]
    qrows = rows_here // SUB
    scale = DH ** (-0.5)
    grads_each = jax.vmap(branch_grads, in_axes=(0, 0, 0, 0, 0, 0, 0, None))
    place = lax.axis_index("kv")
    position = place * rows_here + jnp.arange(rows_here, dtype=jnp.int32)
    gated = gates[..., None] * cotangent.reshape(rows_here, heads, DH).astype(wide)[None]
    delta_all = jnp.sum(gated * branch_out.reshape(2, rows_here, heads, DH).astype(wide), -1)
    delta_all = delta_all.reshape(2, rows_here, groups, group_heads)
    gated_low = gated.astype(jnp.bfloat16).reshape(2, rows_here, groups, group_heads, DH)
    log_all = log_sums.reshape(2, rows_here, groups, group_heads)
    query_all = queries.reshape(rows_here, groups, group_heads, DH)
    pairs = jnp.concatenate(
        [keys.reshape(rows_here, groups, DH), values.reshape(rows_here, groups, DH)], -1
    )
    means = jnp.mean(pairs.reshape(per_summary, CMP, groups, 2 * DH).astype(wide), 1).astype(
        jnp.bfloat16
    )
    summaries = lax.all_gather(means, "kv", axis=0, tiled=True)
    summary_count = summaries.shape[0]
    sum_keys = jnp.transpose(summaries[..., :DH], (1, 0, 2))
    sum_values = jnp.transpose(summaries[..., DH:], (1, 0, 2))
    summary_end = jnp.arange(summary_count, dtype=jnp.int32) * CMP + CMP - 1
    summary_seen = (summary_end[None, :] <= position[:, None])[None]
    query_sum, key_sum, value_sum = branch_grads(
        query_all, sum_keys, sum_values, summary_seen, log_all[0], delta_all[0], gated_low[0], scale
    )
    summary_term = jnp.transpose(jnp.concatenate([key_sum, value_sum], -1), (1, 0, 2))
    listing = lax.dynamic_index_in_dim(chosen, place, 0, keepdims=False)
    live = listing >= 0
    safe = jnp.maximum(listing, 0)
    owner = safe // per_block
    group_index = jnp.arange(groups, dtype=jnp.int32)
    hits = (chosen >= 0) & (chosen // per_block == place)
    wanted = jnp.sum(jnp.where(hits, chosen % per_block, 0), -1)
    asked = jnp.any(hits, -1)
    row_target = safe[..., None] * BLK + jnp.arange(BLK, dtype=jnp.int32)
    pair_blocks = pairs.reshape(per_block, BLK, groups, 2 * DH)
    outbound = pair_blocks[wanted, :, group_index[None, :], :]
    arrived = lax.all_to_all(outbound, "kv", split_axis=0, concat_axis=0, tiled=True)
    picked = arrived[owner, group_index[:, None]]

    def by_sub(array):
        rest = array.shape[3:]
        moved = array.reshape((groups, SUB, TOPN * BLK) + rest)
        return jnp.swapaxes(moved, 0, 1)

    picked_sub = by_sub(picked)
    picked_keys = picked_sub[..., :DH]
    picked_values = picked_sub[..., DH:]
    live_rows = by_sub(jnp.broadcast_to(live[..., None], (groups, nsel, BLK)))
    key_position = by_sub(row_target)
    sub_position = position.reshape(SUB, qrows)
    block_seen = live_rows[:, :, None, :] & (
        key_position[:, :, None, :] <= sub_position[:, None, :, None]
    )
    query_sel, key_sel, value_sel = grads_each(
        query_all.reshape(SUB, qrows, groups, group_heads, DH),
        picked_keys,
        picked_values,
        block_seen,
        log_all[1].reshape(SUB, qrows, groups, group_heads),
        delta_all[1].reshape(SUB, qrows, groups, group_heads),
        gated_low[1].reshape(SUB, qrows, groups, group_heads, DH),
        scale,
    )
    query_sel = query_sel.reshape(rows_here, groups, group_heads, DH)
    key_sel = jnp.swapaxes(key_sel, 0, 1).reshape(groups, nsel, BLK, DH)
    value_sel = jnp.swapaxes(value_sel, 0, 1).reshape(groups, nsel, BLK, DH)
    slot_grads = jnp.concatenate([key_sel, value_sel], -1)
    slot_grads = slot_grads * live[..., None, None].astype(wide)
    outgoing = (
        jnp.zeros((blocks_all, groups, BLK, 2 * DH), wide)
        .at[owner, group_index[:, None]]
        .add(slot_grads)
    )
    summary_out = jnp.transpose(
        summary_term.reshape(blocks_all, per_summary, groups, 2 * DH), (0, 2, 1, 3)
    )
    both_out = jnp.concatenate([outgoing, summary_out], 2)
    both_in = lax.all_to_all(
        both_out.astype(jnp.bfloat16), "kv", split_axis=0, concat_axis=0, tiled=True
    ).astype(both_out.dtype)
    incoming = both_in[:, :, :BLK]
    summary_mine = jnp.transpose(jnp.sum(both_in[:, :, BLK:], 0), (1, 0, 2))
    selector = (
        (wanted[..., None] == jnp.arange(per_block, dtype=jnp.int32)) & asked[..., None]
    ).astype(wide)
    block_sums = jnp.einsum("rgb,rgkc->bkgc", selector, incoming, precision=lax.Precision.HIGHEST)
    pair_grads = (
        block_sums.reshape(rows_here, groups, 2 * DH) + jnp.repeat(summary_mine, CMP, axis=0) / CMP
    )
    grad_queries = (query_sum + query_sel).reshape(rows_here, heads * DH)
    query_low = grad_queries.astype(jnp.bfloat16)
    grad_weight = lax.psum_scatter(
        lax.dot_general(
            hidden, query_low, (((0,), (0,)), ((), ())), preferred_element_type=jnp.float32
        ),
        "kv",
        scatter_dimension=0,
        tiled=True,
    )
    grad_keys = pair_grads[..., :DH].reshape(rows_here, groups * DH)
    grad_values = pair_grads[..., DH:].reshape(rows_here, groups * DH)
    return (grad_queries, grad_keys, grad_values, grad_weight)


WIDE = jnp.float32
LOW = jnp.bfloat16
NT = (((1,), (1,)), ((), ()))
TN = (((0,), (0,)), ((), ()))
NN = (((1,), (0,)), ((), ()))


def dot(a, b, dims):
    return lax.dot_general(a, b, dims, preferred_element_type=WIDE)


def fused_kernel(
    n, q_ref, k_ref, v_ref, hid_ref, log_ref, gate_ref, out_ref, cot_ref, chosen_ref,
    gq_ref, gk_ref, gv_ref, gw_ref,
    table, blk_out, blk_in, grd_out, grd_in, qb_out, qb_in, hid_in, hid_t,
    blk_send, blk_recv, hid_send, hid_recv, qb_send, qb_recv, grd_send, grd_recv, own_sem,
):
    rows, width = q_ref.shape
    heads = width // DH
    lanes = k_ref.shape[1]
    groups = lanes // DH
    group_heads = heads // groups
    per_block = rows // BLK
    per_summary = rows // CMP
    pad = blk_in.shape[1] // 2 - BLK
    qrows = rows // SUB
    cols = hid_in.shape[2]
    scale = DH ** (-0.5)
    me = lax.axis_index("kv")
    to = [lax.rem(me + s, n) for s in range(n)]

    def copy(src, dst, send, recv, peer):
        return pltpu.make_async_remote_copy(
            src_ref=src, dst_ref=dst, send_sem=send, recv_sem=recv,
            device_id={"kv": peer}, device_id_type=pl.DeviceIdType.MESH,
        )

    barrier = pltpu.get_barrier_semaphore()
    for s in range(1, n):
        pl.semaphore_signal(
            barrier, inc=1, device_id={"kv": to[s]}, device_id_type=pl.DeviceIdType.MESH
        )

    def hidden_of(peer):
        return hid_ref.at[:, pl.ds(pl.multiple_of(peer * cols, cols), cols)]

    own_hidden = pltpu.make_async_copy(hidden_of(me), hid_in.at[0], own_sem)
    own_hidden.start()

    lane_group = lax.broadcasted_iota(jnp.int32, (n, lanes), 1) // DH
    wanted = jnp.zeros((n, lanes), WIDE)
    for g in range(groups):
        listing = chosen_ref[:, g, :]
        hit = (listing >= me * per_block) & (listing < (me + 1) * per_block)
        inner = jnp.where(hit, (listing - me * per_block).astype(WIDE), 0.0)
        wanted = jnp.where(lane_group == g, jnp.sum(inner, -1, keepdims=True), wanted)
    table[...] = wanted
    want = [table[pl.ds(to[s], 1), :] for s in range(n)]

    keys = k_ref[...].astype(WIDE)
    values = v_ref[...].astype(WIDE)

    def summary_of(array):
        row = lax.broadcasted_iota(jnp.int32, (pad, lanes), 0)
        result = jnp.zeros((pad, lanes), WIDE)
        for j in range(per_summary):
            mean = jnp.sum(array[j * CMP : (j + 1) * CMP], 0, keepdims=True) / CMP
            result = jnp.where(row == j, mean, result)
        return result.astype(LOW)

    def block_of(array, row):
        result = array[:BLK]
        for b in range(1, per_block):
            result = jnp.where(row == b, array[b * BLK : (b + 1) * BLK], result)
        return result.astype(LOW)

    sum_keys = summary_of(keys)
    sum_values = summary_of(values)
    for s in range(n):
        target = blk_in if s == 0 else blk_out
        target[s, :BLK] = block_of(keys, want[s])
        target[s, BLK : 2 * BLK] = block_of(values, want[s])
        target[s, 2 * BLK : 2 * BLK + pad] = sum_keys
        target[s, 2 * BLK + pad :] = sum_values

    pl.semaphore_wait(barrier, n - 1)
    blk = [
        copy(blk_out.at[s], blk_in.at[s], blk_send.at[s], blk_recv.at[s], to[s]) for s in range(1, n)
    ]
    for c in blk:
        c.start()
    hid = [
        copy(hidden_of(to[s]), hid_in.at[s], hid_send.at[s], hid_recv.at[s], to[s])
        for s in range(1, n)
    ]
    for c in hid:
        c.start()

    def head_stats(branch, h, count):
        at = slice(h * DH, (h + 1) * DH)
        gated = gate_ref[branch, :count, h : h + 1] * cot_ref[:count, at].astype(WIDE)
        delta = jnp.sum(gated * out_ref[branch, :count, at].astype(WIDE), -1, keepdims=True)
        return gated.astype(LOW), delta, log_ref[branch, :count, h : h + 1], q_ref[:count, at]

    def stats(branch, g, count):
        each = [head_stats(branch, g * group_heads + r, count) for r in range(group_heads)]
        return [jnp.concatenate(part, 0) for part in zip(*each)]

    prepared = [(stats(0, g, rows), stats(1, g, qrows)) for g in range(groups)]

    def owner_of(shape, per_slot):
        slot = lax.broadcasted_iota(jnp.int32, shape, 1)
        return lax.rem(me - slot // per_slot + n, n), slot % per_slot

    shape0 = (group_heads * rows, n * pad)
    owner0, inner0 = owner_of(shape0, pad)
    time0 = me * rows + lax.broadcasted_iota(jnp.int32, shape0, 0) % rows
    seen0 = (inner0 < per_summary) & ((owner0 * per_summary + inner0 + 1) * CMP - 1 <= time0)
    shape1 = (group_heads * qrows, n * BLK)
    owner1, inner1 = owner_of(shape1, BLK)
    time1 = lax.broadcasted_iota(jnp.int32, shape1, 0) % qrows

    def branch(query, key, value, seen, low, delta, log):
        probs = jnp.where(seen, jnp.exp(dot(query, key, NT) * scale - log), 0.0)
        score = (probs * (dot(low, value, NT) - delta)).astype(LOW)
        return probs.astype(LOW), score

    for c in blk:
        c.wait_recv()
    all_keys = blk_in[:, :BLK].reshape(n * BLK, lanes)
    all_values = blk_in[:, BLK : 2 * BLK].reshape(n * BLK, lanes)
    all_sum_keys = blk_in[:, 2 * BLK : 2 * BLK + pad].reshape(n * pad, lanes)
    all_sum_values = blk_in[:, 2 * BLK + pad :].reshape(n * pad, lanes)
    probs_all, score_all, grads = [], [], []
    for g in range(groups):
        at = slice(g * DH, (g + 1) * DH)
        (low0, delta0, log0, query0), (low1, delta1, log1, query1) = prepared[g]
        own_block = want[0][:, g * DH : g * DH + 1]
        first = own_block * BLK + inner1.astype(WIDE) <= time1.astype(WIDE)
        seen1 = (owner1 < me) | ((owner1 == me) & first)
        probs0, score0 = branch(query0, all_sum_keys[:, at], all_sum_values[:, at], seen0, low0, delta0, log0)
        probs1, score1 = branch(query1, all_keys[:, at], all_values[:, at], seen1, low1, delta1, log1)
        grad0 = dot(score0, all_sum_keys[:, at], NN) * scale
        grad1 = dot(score1, all_keys[:, at], NN) * scale
        for r in range(group_heads):
            h = slice((g * group_heads + r) * DH, (g * group_heads + r + 1) * DH)
            start = r * rows
            top = grad0[start : start + qrows] + grad1[r * qrows : (r + 1) * qrows]
            gq_ref[:qrows, h] = top
            gq_ref[qrows:, h] = grad0[start + qrows : start + rows]
        probs_all.append((probs0, probs1))
        score_all.append((score0, score1))
    qb_out[...] = gq_ref[...].astype(LOW)
    qb = [copy(qb_out, qb_in.at[s], qb_send.at[s], qb_recv.at[s], to[s]) for s in range(1, n)]

    def wide_of(parts):
        return jnp.concatenate(parts, 1)

    key1 = wide_of([dot(score_all[g][1], prepared[g][1][3], TN) for g in range(groups)]) * scale
    value1 = wide_of([dot(probs_all[g][1], prepared[g][1][0], TN) for g in range(groups)])
    key0 = wide_of([dot(score_all[g][0], prepared[g][0][3], TN) for g in range(groups)]) * scale
    value0 = wide_of([dot(probs_all[g][0], prepared[g][0][0], TN) for g in range(groups)])
    for s in range(1, n):
        grd_out[s, :BLK] = key1[s * BLK : (s + 1) * BLK].astype(LOW)
        grd_out[s, BLK : 2 * BLK] = value1[s * BLK : (s + 1) * BLK].astype(LOW)
        grd_out[s, 2 * BLK : 2 * BLK + pad] = key0[s * pad : (s + 1) * pad].astype(LOW)
        grd_out[s, 2 * BLK + pad :] = value0[s * pad : (s + 1) * pad].astype(LOW)
    grd = [
        copy(grd_out.at[s], grd_in.at[s], grd_send.at[s], grd_recv.at[s], to[n - s])
        for s in range(1, n)
    ]
    for c in qb:
        c.start()
    for c in grd:
        c.start()

    own_hidden.wait()
    hid_t[0] = hid_in[0].T
    total = dot(hid_t[0], qb_out[...], NN)
    for s in range(1, n):
        hid[s - 1].wait_recv()
        hid_t[s] = hid_in[s].T

    for c in grd:
        c.wait_recv()
    for block_part, sum_part, own_block, own_sum, result in (
        (0, 2 * BLK, key1, key0, gk_ref),
        (BLK, 2 * BLK + pad, value1, value0, gv_ref),
    ):
        here = [own_block[:BLK]]
        summed = own_sum[:pad]
        for s in range(1, n):
            here.append(grd_in[s, block_part : block_part + BLK].astype(WIDE))
            summed = summed + grd_in[s, sum_part : sum_part + pad].astype(WIDE)
        for b in range(per_block):
            block = jnp.zeros((BLK, lanes), WIDE)
            for s in range(n):
                block = block + jnp.where(want[s] == b, here[s], 0.0)
            for j in range(BLK // CMP):
                at = b * BLK + j * CMP
                term = summed[at // CMP : at // CMP + 1] / CMP
                result[at : at + CMP] = block[j * CMP : (j + 1) * CMP] + term

    for s in range(1, n):
        qb[s - 1].wait_recv()
        total = total + dot(hid_t[s], qb_in[s], NN)
    gw_ref[...] = total
    for c in blk + hid + qb + grd:
        c.wait_send()


def fused(n, queries, keys, values, hidden, log_sums, gates, branch_out, cotangent, chosen):
    rows, width = queries.shape
    lanes = keys.shape[1]
    cols = hidden.shape[1] // n
    pad = -(-(rows // CMP) // 16) * 16
    size = 2 * (BLK + pad)
    vmem = pl.BlockSpec(memory_space=pltpu.VMEM)
    sems = pltpu.SemaphoreType.DMA((n,))
    return pl.pallas_call(
        functools.partial(fused_kernel, n),
        out_shape=(
            jax.ShapeDtypeStruct((rows, width), WIDE),
            jax.ShapeDtypeStruct((rows, lanes), WIDE),
            jax.ShapeDtypeStruct((rows, lanes), WIDE),
            jax.ShapeDtypeStruct((cols, width), WIDE),
        ),
        in_specs=[vmem] * 3 + [pl.BlockSpec(memory_space=pl.ANY)] + [vmem] * 5,
        out_specs=(vmem,) * 4,
        scratch_shapes=[
            pltpu.VMEM((n, lanes), WIDE),
            pltpu.VMEM((n, size, lanes), LOW),
            pltpu.VMEM((n, size, lanes), LOW),
            pltpu.VMEM((n, size, lanes), LOW),
            pltpu.VMEM((n, size, lanes), LOW),
            pltpu.VMEM((rows, width), LOW),
            pltpu.VMEM((n, rows, width), LOW),
            pltpu.VMEM((n, rows, cols), LOW),
            pltpu.VMEM((n, cols, rows), LOW),
            sems, sems, sems, sems, sems, sems, sems, sems,
            pltpu.SemaphoreType.DMA,
        ],
        compiler_params=pltpu.CompilerParams(collective_id=0, has_side_effects=True),
    )(queries, keys, values, hidden, log_sums, gates, branch_out, cotangent, chosen)


def fits(n, hidden, chosen):
    return chosen.shape[0] <= TOPN and (hidden.shape[1] // n) % 128 == 0


def solution(mesh):

    n = mesh.shape["kv"]

    def body(*args):
        return fused(n, *args) if fits(n, args[3], args[8]) else shards(*args)

    return jax.shard_map(
        body,
        mesh=mesh,
        in_specs=(
            P("kv", "tp"),
            P("kv", "tp"),
            P("kv", "tp"),
            P("kv", None),
            P(None, "kv", "tp"),
            P(None, "kv", "tp"),
            P(None, "kv", "tp"),
            P("kv", "tp"),
            P(None, "tp", None),
        ),
        out_specs=(P("kv", "tp"), P("kv", "tp"), P("kv", "tp"), P("kv", "tp")),
        check_vma=False,
    )
```

```python
import functools

import jax
import jax.numpy as jnp
from jax import lax
from jax.experimental import pallas as pl
from jax.experimental.pallas import tpu as pltpu
from jax.sharding import PartitionSpec as P

DH = 64
BLK = 32
TOPN = 12
SUB = 4
CMP = 32


def branch_grads(query_rows, key_rows, value_rows, seen, log_rows, delta_rows, cot_rows, scale):
    wide = jnp.float32
    scores = jnp.einsum("tgre,gme->grtm", query_rows, key_rows, preferred_element_type=wide) * scale
    log_here = jnp.transpose(log_rows, (1, 2, 0))[..., None]
    delta_here = jnp.transpose(delta_rows, (1, 2, 0))[..., None]
    probs = jnp.where(seen[:, None], jnp.exp(scores - log_here), 0.0)
    probs_low = probs.astype(jnp.bfloat16)
    value_grad = jnp.einsum("grtm,tgre->gme", probs_low, cot_rows, preferred_element_type=wide)
    prob_grad = jnp.einsum("tgre,gme->grtm", cot_rows, value_rows, preferred_element_type=wide)
    score_low = (probs * (prob_grad - delta_here)).astype(jnp.bfloat16)
    query_grad = (
        jnp.einsum("grtm,gme->tgre", score_low, key_rows, preferred_element_type=wide) * scale
    )
    key_grad = (
        jnp.einsum("grtm,tgre->gme", score_low, query_rows, preferred_element_type=wide) * scale
    )
    return (query_grad, key_grad, value_grad)


def shards(queries, keys, values, hidden, log_sums, gates, branch_out, cotangent, chosen):
    wide = jnp.float32
    rows_here = queries.shape[0]
    heads = queries.shape[1] // DH
    groups = keys.shape[1] // DH
    group_heads = heads // groups
    per_block = rows_here // BLK
    per_summary = rows_here // CMP
    blocks_all = chosen.shape[0]
    nsel = chosen.shape[2]
    qrows = rows_here // SUB
    scale = DH ** (-0.5)
    grads_each = jax.vmap(branch_grads, in_axes=(0, 0, 0, 0, 0, 0, 0, None))
    place = lax.axis_index("kv")
    position = place * rows_here + jnp.arange(rows_here, dtype=jnp.int32)
    gated = gates[..., None] * cotangent.reshape(rows_here, heads, DH).astype(wide)[None]
    delta_all = jnp.sum(gated * branch_out.reshape(2, rows_here, heads, DH).astype(wide), -1)
    delta_all = delta_all.reshape(2, rows_here, groups, group_heads)
    gated_low = gated.astype(jnp.bfloat16).reshape(2, rows_here, groups, group_heads, DH)
    log_all = log_sums.reshape(2, rows_here, groups, group_heads)
    query_all = queries.reshape(rows_here, groups, group_heads, DH)
    pairs = jnp.concatenate(
        [keys.reshape(rows_here, groups, DH), values.reshape(rows_here, groups, DH)], -1
    )
    means = jnp.mean(pairs.reshape(per_summary, CMP, groups, 2 * DH).astype(wide), 1).astype(
        jnp.bfloat16
    )
    summaries = lax.all_gather(means, "kv", axis=0, tiled=True)
    summary_count = summaries.shape[0]
    sum_keys = jnp.transpose(summaries[..., :DH], (1, 0, 2))
    sum_values = jnp.transpose(summaries[..., DH:], (1, 0, 2))
    summary_end = jnp.arange(summary_count, dtype=jnp.int32) * CMP + CMP - 1
    summary_seen = (summary_end[None, :] <= position[:, None])[None]
    query_sum, key_sum, value_sum = branch_grads(
        query_all, sum_keys, sum_values, summary_seen, log_all[0], delta_all[0], gated_low[0], scale
    )
    summary_term = jnp.transpose(jnp.concatenate([key_sum, value_sum], -1), (1, 0, 2))
    listing = lax.dynamic_index_in_dim(chosen, place, 0, keepdims=False)
    live = listing >= 0
    safe = jnp.maximum(listing, 0)
    owner = safe // per_block
    group_index = jnp.arange(groups, dtype=jnp.int32)
    hits = (chosen >= 0) & (chosen // per_block == place)
    wanted = jnp.sum(jnp.where(hits, chosen % per_block, 0), -1)
    asked = jnp.any(hits, -1)
    row_target = safe[..., None] * BLK + jnp.arange(BLK, dtype=jnp.int32)
    pair_blocks = pairs.reshape(per_block, BLK, groups, 2 * DH)
    outbound = pair_blocks[wanted, :, group_index[None, :], :]
    arrived = lax.all_to_all(outbound, "kv", split_axis=0, concat_axis=0, tiled=True)
    picked = arrived[owner, group_index[:, None]]

    def by_sub(array):
        rest = array.shape[3:]
        moved = array.reshape((groups, SUB, TOPN * BLK) + rest)
        return jnp.swapaxes(moved, 0, 1)

    picked_sub = by_sub(picked)
    picked_keys = picked_sub[..., :DH]
    picked_values = picked_sub[..., DH:]
    live_rows = by_sub(jnp.broadcast_to(live[..., None], (groups, nsel, BLK)))
    key_position = by_sub(row_target)
    sub_position = position.reshape(SUB, qrows)
    block_seen = live_rows[:, :, None, :] & (
        key_position[:, :, None, :] <= sub_position[:, None, :, None]
    )
    query_sel, key_sel, value_sel = grads_each(
        query_all.reshape(SUB, qrows, groups, group_heads, DH),
        picked_keys,
        picked_values,
        block_seen,
        log_all[1].reshape(SUB, qrows, groups, group_heads),
        delta_all[1].reshape(SUB, qrows, groups, group_heads),
        gated_low[1].reshape(SUB, qrows, groups, group_heads, DH),
        scale,
    )
    query_sel = query_sel.reshape(rows_here, groups, group_heads, DH)
    key_sel = jnp.swapaxes(key_sel, 0, 1).reshape(groups, nsel, BLK, DH)
    value_sel = jnp.swapaxes(value_sel, 0, 1).reshape(groups, nsel, BLK, DH)
    slot_grads = jnp.concatenate([key_sel, value_sel], -1)
    slot_grads = slot_grads * live[..., None, None].astype(wide)
    outgoing = (
        jnp.zeros((blocks_all, groups, BLK, 2 * DH), wide)
        .at[owner, group_index[:, None]]
        .add(slot_grads)
    )
    summary_out = jnp.transpose(
        summary_term.reshape(blocks_all, per_summary, groups, 2 * DH), (0, 2, 1, 3)
    )
    both_out = jnp.concatenate([outgoing, summary_out], 2)
    both_in = lax.all_to_all(
        both_out.astype(jnp.bfloat16), "kv", split_axis=0, concat_axis=0, tiled=True
    ).astype(both_out.dtype)
    incoming = both_in[:, :, :BLK]
    summary_mine = jnp.transpose(jnp.sum(both_in[:, :, BLK:], 0), (1, 0, 2))
    selector = (
        (wanted[..., None] == jnp.arange(per_block, dtype=jnp.int32)) & asked[..., None]
    ).astype(wide)
    block_sums = jnp.einsum("rgb,rgkc->bkgc", selector, incoming, precision=lax.Precision.HIGHEST)
    pair_grads = (
        block_sums.reshape(rows_here, groups, 2 * DH) + jnp.repeat(summary_mine, CMP, axis=0) / CMP
    )
    grad_queries = (query_sum + query_sel).reshape(rows_here, heads * DH)
    query_low = grad_queries.astype(jnp.bfloat16)
    grad_weight = lax.psum_scatter(
        lax.dot_general(
            hidden, query_low, (((0,), (0,)), ((), ())), preferred_element_type=jnp.float32
        ),
        "kv",
        scatter_dimension=0,
        tiled=True,
    )
    grad_keys = pair_grads[..., :DH].reshape(rows_here, groups * DH)
    grad_values = pair_grads[..., DH:].reshape(rows_here, groups * DH)
    return (grad_queries, grad_keys, grad_values, grad_weight)


WIDE = jnp.float32
LOW = jnp.bfloat16
NT = (((1,), (1,)), ((), ()))
TN = (((0,), (0,)), ((), ()))
NN = (((1,), (0,)), ((), ()))


def dot(a, b, dims):
    return lax.dot_general(a, b, dims, preferred_element_type=WIDE)


def fused_kernel(
    n, tps, q_ref, k_ref, v_ref, hid_ref, log_ref, gate_ref, out_ref, cot_ref, chosen_ref,
    gq_ref, gk_ref, gv_ref, gw_ref,
    table, blk_out, blk_in, grd_out, grd_in, qb_out, qb_in, hid_in, hid_t,
    blk_send, blk_recv, hid_send, hid_recv, qb_send, qb_recv, grd_send, grd_recv,
    pass_send, pass_recv, share_send, share_recv, own_sem,
):
    rows, width = q_ref.shape
    heads = width // DH
    lanes = k_ref.shape[1]
    groups = lanes // DH
    group_heads = heads // groups
    per_block = rows // BLK
    per_summary = rows // CMP
    pad = (blk_in.shape[1] - 2 * BLK) // 2
    qrows = rows // SUB
    cols = hid_in.shape[2]
    part = rows // tps
    scale = DH ** (-0.5)
    me = lax.axis_index("kv")
    my_tp = lax.axis_index("tp")
    half = n // 2
    place, side = me // 2, me % 2
    to = [2 * lax.rem(place + s // 2, half) + lax.rem(side + s % 2, 2) for s in range(n)]
    come = [2 * lax.rem(place + half - s // 2, half) + lax.rem(side + s % 2, 2) for s in range(n)]
    mesh_id = pl.DeviceIdType.MESH

    def copy(src, dst, send, recv, **peer):
        return pltpu.make_async_remote_copy(
            src_ref=src, dst_ref=dst, send_sem=send, recv_sem=recv,
            device_id=peer, device_id_type=mesh_id,
        )

    barrier = pltpu.get_barrier_semaphore()
    for s in range(n - 1, 0, -1):
        pl.semaphore_signal(barrier, inc=1, device_id={"kv": to[s]}, device_id_type=mesh_id)
    tp_to = [lax.rem(my_tp + u, tps) for u in range(tps)]
    for u in range(1, tps):
        pl.semaphore_signal(barrier, inc=1, device_id={"tp": tp_to[u]}, device_id_type=mesh_id)

    part_rows = pl.ds(pl.multiple_of(my_tp * part, part), part)

    def hidden_of(peer):
        return hid_ref.at[part_rows, pl.ds(pl.multiple_of(peer * cols, cols), cols)]

    own_hidden = pltpu.make_async_copy(hidden_of(me), hid_in.at[0, part_rows], own_sem)
    own_hidden.start()

    lane_group = lax.broadcasted_iota(jnp.int32, (n, lanes), 1) // DH
    wanted = jnp.zeros((n, lanes), WIDE)
    for g in range(groups):
        listing = chosen_ref[:, g, :]
        hit = (listing >= me * per_block) & (listing < (me + 1) * per_block)
        inner = jnp.where(hit, (listing - me * per_block).astype(WIDE), 0.0)
        wanted = jnp.where(lane_group == g, jnp.sum(inner, -1, keepdims=True), wanted)
    table[...] = wanted
    want = [table[pl.ds(to[s], 1), :] for s in range(n)]

    keys = k_ref[...].astype(WIDE)
    values = v_ref[...].astype(WIDE)

    def summary_of(array):
        row = lax.broadcasted_iota(jnp.int32, (pad, lanes), 0)
        result = jnp.zeros((pad, lanes), WIDE)
        for j in range(per_summary):
            mean = jnp.sum(array[j * CMP : (j + 1) * CMP], 0, keepdims=True) / CMP
            result = jnp.where(row == j, mean, result)
        return result

    def block_of(array, row):
        result = array[:BLK]
        for b in range(1, per_block):
            result = jnp.where(row == b, array[b * BLK : (b + 1) * BLK], result)
        return result.astype(LOW)

    sums = jnp.concatenate([summary_of(keys), summary_of(values)], 0).astype(LOW)
    for s in range(n):
        target = blk_in if s == 0 else blk_out
        target[s, :BLK] = block_of(keys, want[s])
        target[s, BLK : 2 * BLK] = block_of(values, want[s])
        target[s, 2 * BLK :] = sums

    pl.semaphore_wait(barrier, n - 1 + tps - 1)
    blk = [
        copy(blk_out.at[s], blk_in.at[s], blk_send.at[s], blk_recv.at[s], kv=to[s]) for s in range(1, n)
    ]
    for c in blk:
        c.start()
    hid = [
        copy(hidden_of(to[s]), hid_in.at[s, part_rows], hid_send.at[s], hid_recv.at[s], kv=to[s])
        for s in range(1, n)
    ]
    for c in hid:
        c.start()

    columns = jnp.concatenate([log_ref[0], log_ref[1], gate_ref[0], gate_ref[1]], 0).T

    def column(kind, branch, h, count):
        at = (2 * kind + branch) * heads + h
        return columns[:count, at : at + 1]

    def head_stats(branch, h, count):
        at = slice(h * DH, (h + 1) * DH)
        gated = column(1, branch, h, count) * cot_ref[:count, at].astype(WIDE)
        delta = jnp.sum(gated * out_ref[branch, :count, at].astype(WIDE), -1, keepdims=True)
        return gated.astype(LOW), delta, column(0, branch, h, count), q_ref[:count, at]

    def stats(branch, g, count):
        each = [head_stats(branch, g * group_heads + r, count) for r in range(group_heads)]
        return [jnp.concatenate(piece, 0) for piece in zip(*each)]

    prepared = [(stats(0, g, rows), stats(1, g, qrows)) for g in range(groups)]

    def owner_of(shape, per_slot):
        column_at = lax.broadcasted_iota(jnp.int32, shape, 1)
        slot = column_at // per_slot
        owner = 2 * lax.rem(place + half - slot // 2, half) + lax.rem(side + slot % 2, 2)
        return owner, column_at % per_slot

    shape0 = (group_heads * rows, n * pad)
    owner0, inner0 = owner_of(shape0, pad)
    time0 = me * rows + lax.broadcasted_iota(jnp.int32, shape0, 0) % rows
    seen0 = (inner0 < per_summary) & ((owner0 * per_summary + inner0 + 1) * CMP - 1 <= time0)
    shape1 = (group_heads * qrows, n * BLK)
    owner1, inner1 = owner_of(shape1, BLK)
    time1 = lax.broadcasted_iota(jnp.int32, shape1, 0) % qrows

    def branch(query, key, value, seen, low, delta, log):
        probs = jnp.where(seen, jnp.exp(dot(query, key, NT) * scale - log), 0.0)
        score = (probs * (dot(low, value, NT) - delta)).astype(LOW)
        return probs.astype(LOW), score

    for c in blk:
        c.wait_recv()
    all_keys = blk_in[:, :BLK].reshape(n * BLK, lanes)
    all_values = blk_in[:, BLK : 2 * BLK].reshape(n * BLK, lanes)
    all_sums = blk_in[:, 2 * BLK :].astype(WIDE)
    all_sum_keys = all_sums[:, :pad].reshape(n * pad, lanes).astype(LOW)
    all_sum_values = all_sums[:, pad:].reshape(n * pad, lanes).astype(LOW)
    probs_all, score_all = [], []
    for g in range(groups):
        at = slice(g * DH, (g + 1) * DH)
        (low0, delta0, log0, query0), (low1, delta1, log1, query1) = prepared[g]
        own_block = want[0][:, g * DH : g * DH + 1]
        first = own_block * BLK + inner1.astype(WIDE) <= time1.astype(WIDE)
        seen1 = (owner1 < me) | ((owner1 == me) & first)
        probs0, score0 = branch(query0, all_sum_keys[:, at], all_sum_values[:, at], seen0, low0, delta0, log0)
        probs1, score1 = branch(query1, all_keys[:, at], all_values[:, at], seen1, low1, delta1, log1)
        grad0 = dot(score0, all_sum_keys[:, at], NN) * scale
        grad1 = dot(score1, all_keys[:, at], NN) * scale
        for r in range(group_heads):
            h = slice((g * group_heads + r) * DH, (g * group_heads + r + 1) * DH)
            start = r * rows
            top = grad0[start : start + qrows] + grad1[r * qrows : (r + 1) * qrows]
            gq_ref[:qrows, h] = top
            gq_ref[qrows:, h] = grad0[start + qrows : start + rows]
        probs_all.append((probs0, probs1))
        score_all.append((score0, score1))
    qb_out[...] = gq_ref[...].astype(LOW)
    direct = [s for s in range(1, n) if s % 2 == 0 or s == 1]
    qb = {
        s: copy(qb_out, qb_in.at[s], qb_send.at[s], qb_recv.at[s], kv=to[s]) for s in direct
    }
    passed = {
        s: copy(qb_in.at[s], qb_in.at[s + 1], pass_send.at[s], pass_recv.at[s], kv=to[1])
        for s in range(2, n, 2)
    }
    for s in reversed(direct):
        qb[s].start()

    def wide_of(parts):
        return jnp.concatenate(parts, 1)

    key1 = wide_of([dot(score_all[g][1], prepared[g][1][3], TN) for g in range(groups)]) * scale
    value1 = wide_of([dot(probs_all[g][1], prepared[g][1][0], TN) for g in range(groups)])
    key0 = wide_of([dot(score_all[g][0], prepared[g][0][3], TN) for g in range(groups)]) * scale
    value0 = wide_of([dot(probs_all[g][0], prepared[g][0][0], TN) for g in range(groups)])
    for s in range(1, n):
        grd_out[s, :BLK] = key1[s * BLK : (s + 1) * BLK].astype(LOW)
        grd_out[s, BLK : 2 * BLK] = value1[s * BLK : (s + 1) * BLK].astype(LOW)
        both = [key0[s * pad : (s + 1) * pad], value0[s * pad : (s + 1) * pad]]
        grd_out[s, 2 * BLK :] = jnp.concatenate(both, 0).astype(LOW)
    grd = [
        copy(grd_out.at[s], grd_in.at[s], grd_send.at[s], grd_recv.at[s], kv=come[s])
        for s in range(1, n)
    ]
    for c in grd:
        c.start()

    own_hidden.wait()
    for c in hid:
        c.wait_recv()
    mine = hid_in.at[:, part_rows]
    share = [
        copy(mine, mine, share_send.at[u], share_recv.at[u], tp=tp_to[u]) for u in range(1, tps)
    ]
    for c in share:
        c.start()

    for s in range(2, n, 2):
        qb[s].wait_recv()
        passed[s].start()

    for c in grd:
        c.wait_recv()
    for block_part, sum_part, own_block, own_sum, result in (
        (0, 0, key1, key0, gk_ref),
        (BLK, pad, value1, value0, gv_ref),
    ):
        here = [own_block[:BLK]]
        summed = own_sum[:pad]
        for s in range(1, n):
            here.append(grd_in[s, block_part : block_part + BLK].astype(WIDE))
            summed = summed + grd_in[s, 2 * BLK :].astype(WIDE)[sum_part : sum_part + pad]
        for b in range(per_block):
            block = jnp.zeros((BLK, lanes), WIDE)
            for s in range(n):
                block = block + jnp.where(want[s] == b, here[s], 0.0)
            for j in range(BLK // CMP):
                at = b * BLK + j * CMP
                term = summed[at // CMP : at // CMP + 1] / CMP
                result[at : at + CMP] = block[j * CMP : (j + 1) * CMP] + term

    for u in range(1, tps):
        other = lax.rem(my_tp + tps - u, tps)
        arrived = hid_in.at[:, pl.ds(pl.multiple_of(other * part, part), part)]
        copy(mine, arrived, share_send.at[u], share_recv.at[u], tp=tp_to[u]).wait_recv()
    for s in range(n):
        hid_t[s] = hid_in[s].T
    total = dot(hid_t[0], qb_out[...], NN)
    for s in range(2, n, 2):
        total = total + dot(hid_t[s], qb_in[s], NN)
    qb[1].wait_recv()
    total = total + dot(hid_t[1], qb_in[1], NN)
    for s in range(2, n, 2):
        passed[s].wait_recv()
        total = total + dot(hid_t[s + 1], qb_in[s + 1], NN)
    gw_ref[...] = total
    for c in blk + hid + list(qb.values()) + grd + share + list(passed.values()):
        c.wait_send()


def fused(n, tps, queries, keys, values, hidden, log_sums, gates, branch_out, cotangent, chosen):
    rows, width = queries.shape
    lanes = keys.shape[1]
    cols = hidden.shape[1] // n
    pad = -(-(rows // CMP) // 8) * 8
    size = 2 * (BLK + pad)
    vmem = pl.BlockSpec(memory_space=pltpu.VMEM)
    sems = pltpu.SemaphoreType.DMA((n,))
    tp_sems = pltpu.SemaphoreType.DMA((tps,))
    return pl.pallas_call(
        functools.partial(fused_kernel, n, tps),
        out_shape=(
            jax.ShapeDtypeStruct((rows, width), WIDE),
            jax.ShapeDtypeStruct((rows, lanes), WIDE),
            jax.ShapeDtypeStruct((rows, lanes), WIDE),
            jax.ShapeDtypeStruct((cols, width), WIDE),
        ),
        in_specs=[vmem] * 3 + [pl.BlockSpec(memory_space=pl.ANY)] + [vmem] * 5,
        out_specs=(vmem,) * 4,
        scratch_shapes=[
            pltpu.VMEM((n, lanes), WIDE),
            pltpu.VMEM((n, size, lanes), LOW),
            pltpu.VMEM((n, size, lanes), LOW),
            pltpu.VMEM((n, size, lanes), LOW),
            pltpu.VMEM((n, size, lanes), LOW),
            pltpu.VMEM((rows, width), LOW),
            pltpu.VMEM((n, rows, width), LOW),
            pltpu.VMEM((n, rows, cols), LOW),
            pltpu.VMEM((n, cols, rows), LOW),
            sems, sems, sems, sems, sems, sems, sems, sems, sems, sems,
            tp_sems, tp_sems,
            pltpu.SemaphoreType.DMA,
        ],
        compiler_params=pltpu.CompilerParams(collective_id=0, has_side_effects=True),
    )(
        queries, keys, values, hidden, jnp.swapaxes(log_sums, 1, 2), jnp.swapaxes(gates, 1, 2),
        branch_out, cotangent, chosen,
    )


def fits(n, tps, hidden, chosen):
    whole = (hidden.shape[1] // n) % 128 == 0 and (hidden.shape[0] // tps) % 16 == 0
    return chosen.shape[0] <= TOPN and n % 2 == 0 and whole


def solution(mesh):

    n, tps = mesh.shape["kv"], mesh.shape["tp"]

    def body(*args):
        return fused(n, tps, *args) if fits(n, tps, args[3], args[8]) else shards(*args)

    return jax.shard_map(
        body,
        mesh=mesh,
        in_specs=(
            P("kv", "tp"),
            P("kv", "tp"),
            P("kv", "tp"),
            P("kv", None),
            P(None, "kv", "tp"),
            P(None, "kv", "tp"),
            P(None, "kv", "tp"),
            P("kv", "tp"),
            P(None, "tp", None),
        ),
        out_specs=(P("kv", "tp"), P("kv", "tp"), P("kv", "tp"), P("kv", "tp")),
        check_vma=False,
    )
```

```python
import functools

import jax
import jax.numpy as jnp
from jax import lax
from jax.experimental import pallas as pl
from jax.experimental.pallas import tpu as pltpu
from jax.sharding import PartitionSpec as P

DH = 64
BLK = 32
TOPN = 12
SUB = 4
CMP = 32


def branch_grads(query_rows, key_rows, value_rows, seen, log_rows, delta_rows, cot_rows, scale):
    wide = jnp.float32
    scores = jnp.einsum("tgre,gme->grtm", query_rows, key_rows, preferred_element_type=wide) * scale
    log_here = jnp.transpose(log_rows, (1, 2, 0))[..., None]
    delta_here = jnp.transpose(delta_rows, (1, 2, 0))[..., None]
    probs = jnp.where(seen[:, None], jnp.exp(scores - log_here), 0.0)
    probs_low = probs.astype(jnp.bfloat16)
    value_grad = jnp.einsum("grtm,tgre->gme", probs_low, cot_rows, preferred_element_type=wide)
    prob_grad = jnp.einsum("tgre,gme->grtm", cot_rows, value_rows, preferred_element_type=wide)
    score_low = (probs * (prob_grad - delta_here)).astype(jnp.bfloat16)
    query_grad = (
        jnp.einsum("grtm,gme->tgre", score_low, key_rows, preferred_element_type=wide) * scale
    )
    key_grad = (
        jnp.einsum("grtm,tgre->gme", score_low, query_rows, preferred_element_type=wide) * scale
    )
    return (query_grad, key_grad, value_grad)


def shards(queries, keys, values, hidden, log_sums, gates, branch_out, cotangent, chosen):
    wide = jnp.float32
    rows_here = queries.shape[0]
    heads = queries.shape[1] // DH
    groups = keys.shape[1] // DH
    group_heads = heads // groups
    per_block = rows_here // BLK
    per_summary = rows_here // CMP
    blocks_all = chosen.shape[0]
    nsel = chosen.shape[2]
    qrows = rows_here // SUB
    scale = DH ** (-0.5)
    grads_each = jax.vmap(branch_grads, in_axes=(0, 0, 0, 0, 0, 0, 0, None))
    place = lax.axis_index("kv")
    position = place * rows_here + jnp.arange(rows_here, dtype=jnp.int32)
    gated = gates[..., None] * cotangent.reshape(rows_here, heads, DH).astype(wide)[None]
    delta_all = jnp.sum(gated * branch_out.reshape(2, rows_here, heads, DH).astype(wide), -1)
    delta_all = delta_all.reshape(2, rows_here, groups, group_heads)
    gated_low = gated.astype(jnp.bfloat16).reshape(2, rows_here, groups, group_heads, DH)
    log_all = log_sums.reshape(2, rows_here, groups, group_heads)
    query_all = queries.reshape(rows_here, groups, group_heads, DH)
    pairs = jnp.concatenate(
        [keys.reshape(rows_here, groups, DH), values.reshape(rows_here, groups, DH)], -1
    )
    means = jnp.mean(pairs.reshape(per_summary, CMP, groups, 2 * DH).astype(wide), 1).astype(
        jnp.bfloat16
    )
    summaries = lax.all_gather(means, "kv", axis=0, tiled=True)
    summary_count = summaries.shape[0]
    sum_keys = jnp.transpose(summaries[..., :DH], (1, 0, 2))
    sum_values = jnp.transpose(summaries[..., DH:], (1, 0, 2))
    summary_end = jnp.arange(summary_count, dtype=jnp.int32) * CMP + CMP - 1
    summary_seen = (summary_end[None, :] <= position[:, None])[None]
    query_sum, key_sum, value_sum = branch_grads(
        query_all, sum_keys, sum_values, summary_seen, log_all[0], delta_all[0], gated_low[0], scale
    )
    summary_term = jnp.transpose(jnp.concatenate([key_sum, value_sum], -1), (1, 0, 2))
    listing = lax.dynamic_index_in_dim(chosen, place, 0, keepdims=False)
    live = listing >= 0
    safe = jnp.maximum(listing, 0)
    owner = safe // per_block
    group_index = jnp.arange(groups, dtype=jnp.int32)
    hits = (chosen >= 0) & (chosen // per_block == place)
    wanted = jnp.sum(jnp.where(hits, chosen % per_block, 0), -1)
    asked = jnp.any(hits, -1)
    row_target = safe[..., None] * BLK + jnp.arange(BLK, dtype=jnp.int32)
    pair_blocks = pairs.reshape(per_block, BLK, groups, 2 * DH)
    outbound = pair_blocks[wanted, :, group_index[None, :], :]
    arrived = lax.all_to_all(outbound, "kv", split_axis=0, concat_axis=0, tiled=True)
    picked = arrived[owner, group_index[:, None]]

    def by_sub(array):
        rest = array.shape[3:]
        moved = array.reshape((groups, SUB, TOPN * BLK) + rest)
        return jnp.swapaxes(moved, 0, 1)

    picked_sub = by_sub(picked)
    picked_keys = picked_sub[..., :DH]
    picked_values = picked_sub[..., DH:]
    live_rows = by_sub(jnp.broadcast_to(live[..., None], (groups, nsel, BLK)))
    key_position = by_sub(row_target)
    sub_position = position.reshape(SUB, qrows)
    block_seen = live_rows[:, :, None, :] & (
        key_position[:, :, None, :] <= sub_position[:, None, :, None]
    )
    query_sel, key_sel, value_sel = grads_each(
        query_all.reshape(SUB, qrows, groups, group_heads, DH),
        picked_keys,
        picked_values,
        block_seen,
        log_all[1].reshape(SUB, qrows, groups, group_heads),
        delta_all[1].reshape(SUB, qrows, groups, group_heads),
        gated_low[1].reshape(SUB, qrows, groups, group_heads, DH),
        scale,
    )
    query_sel = query_sel.reshape(rows_here, groups, group_heads, DH)
    key_sel = jnp.swapaxes(key_sel, 0, 1).reshape(groups, nsel, BLK, DH)
    value_sel = jnp.swapaxes(value_sel, 0, 1).reshape(groups, nsel, BLK, DH)
    slot_grads = jnp.concatenate([key_sel, value_sel], -1)
    slot_grads = slot_grads * live[..., None, None].astype(wide)
    outgoing = (
        jnp.zeros((blocks_all, groups, BLK, 2 * DH), wide)
        .at[owner, group_index[:, None]]
        .add(slot_grads)
    )
    summary_out = jnp.transpose(
        summary_term.reshape(blocks_all, per_summary, groups, 2 * DH), (0, 2, 1, 3)
    )
    both_out = jnp.concatenate([outgoing, summary_out], 2)
    both_in = lax.all_to_all(
        both_out.astype(jnp.bfloat16), "kv", split_axis=0, concat_axis=0, tiled=True
    ).astype(both_out.dtype)
    incoming = both_in[:, :, :BLK]
    summary_mine = jnp.transpose(jnp.sum(both_in[:, :, BLK:], 0), (1, 0, 2))
    selector = (
        (wanted[..., None] == jnp.arange(per_block, dtype=jnp.int32)) & asked[..., None]
    ).astype(wide)
    block_sums = jnp.einsum("rgb,rgkc->bkgc", selector, incoming, precision=lax.Precision.HIGHEST)
    pair_grads = (
        block_sums.reshape(rows_here, groups, 2 * DH) + jnp.repeat(summary_mine, CMP, axis=0) / CMP
    )
    grad_queries = (query_sum + query_sel).reshape(rows_here, heads * DH)
    query_low = grad_queries.astype(jnp.bfloat16)
    grad_weight = lax.psum_scatter(
        lax.dot_general(
            hidden, query_low, (((0,), (0,)), ((), ())), preferred_element_type=jnp.float32
        ),
        "kv",
        scatter_dimension=0,
        tiled=True,
    )
    grad_keys = pair_grads[..., :DH].reshape(rows_here, groups * DH)
    grad_values = pair_grads[..., DH:].reshape(rows_here, groups * DH)
    return (grad_queries, grad_keys, grad_values, grad_weight)


WIDE = jnp.float32
LOW = jnp.bfloat16
NT = (((1,), (1,)), ((), ()))
TN = (((0,), (0,)), ((), ()))
NN = (((1,), (0,)), ((), ()))


def dot(a, b, dims):
    return lax.dot_general(a, b, dims, preferred_element_type=WIDE)


def fused_kernel(
    n, tps, q_hbm, k_hbm, v_hbm, hid_ref, log_hbm, gate_hbm, out_hbm, cot_hbm, chosen_hbm,
    gq_ref, gk_ref, gv_ref, gw_ref,
    k_ref, v_ref, chosen_ref, q_ref, cot_ref, gate_ref, out_ref, log_ref,
    table, sum_out, sum_in, blk_out, blk_in, grd_out, grd_in, qb_out, qb_in, hid_in, hid_t,
    sum_send, sum_recv, blk_send, blk_recv, hid_send, hid_recv, qb_send, qb_recv,
    grd_send, grd_recv, pass_send, pass_recv, share_send, share_recv, own_sem, load_sem,
):
    rows, width = q_ref.shape
    heads = width // DH
    lanes = k_ref.shape[1]
    groups = lanes // DH
    group_heads = heads // groups
    per_block = rows // BLK
    per_summary = rows // CMP
    pad = sum_in.shape[1] // 2
    qrows = rows // SUB
    cols = hid_in.shape[2]
    part = rows // tps
    scale = DH ** (-0.5)
    me = lax.axis_index("kv")
    my_tp = lax.axis_index("tp")
    half = n // 2
    place, side = me // 2, me % 2
    to = [2 * lax.rem(place + s // 2, half) + lax.rem(side + s % 2, 2) for s in range(n)]
    come = [2 * lax.rem(place + half - s // 2, half) + lax.rem(side + s % 2, 2) for s in range(n)]
    mesh_id = pl.DeviceIdType.MESH

    def copy(src, dst, send, recv, **peer):
        return pltpu.make_async_remote_copy(
            src_ref=src, dst_ref=dst, send_sem=send, recv_sem=recv,
            device_id=peer, device_id_type=mesh_id,
        )

    pairs = (
        (k_hbm, k_ref), (v_hbm, v_ref), (chosen_hbm, chosen_ref), (q_hbm, q_ref),
        (cot_hbm, cot_ref), (gate_hbm, gate_ref), (out_hbm, out_ref), (log_hbm, log_ref),
    )
    loads = [pltpu.make_async_copy(*pair, load_sem.at[i]) for i, pair in enumerate(pairs)]
    barrier = pltpu.get_barrier_semaphore()
    for s in range(n - 1, 0, -1):
        pl.semaphore_signal(barrier, inc=1, device_id={"kv": to[s]}, device_id_type=mesh_id)
    tp_to = [lax.rem(my_tp + u, tps) for u in range(tps)]
    for u in range(1, tps):
        pl.semaphore_signal(barrier, inc=1, device_id={"tp": tp_to[u]}, device_id_type=mesh_id)

    for c in loads:
        c.start()
    later = [to[s] > me for s in range(n)]
    earlier = [come[s] < me for s in range(n)]

    def each(copies, conditions, act):
        for c, condition in zip(copies, conditions[1:]):
            pl.when(condition)(functools.partial(act, c))

    for s in range(1, n):

        @pl.when(jnp.logical_not(earlier[s]))
        def _():
            blk_in[s] = jnp.zeros(blk_in.shape[1:], LOW)

        @pl.when(jnp.logical_not(later[s]))
        def _():
            grd_in[s] = jnp.zeros(grd_in.shape[1:], LOW)

    part_rows = pl.ds(pl.multiple_of(my_tp * part, part), part)

    def hidden_of(peer):
        return hid_ref.at[part_rows, pl.ds(pl.multiple_of(peer * cols, cols), cols)]

    own_hidden = pltpu.make_async_copy(hidden_of(me), hid_in.at[0, part_rows], own_sem)
    own_hidden.start()

    for c in loads[:3]:
        c.wait()
    lane_group = lax.broadcasted_iota(jnp.int32, (n, lanes), 1) // DH
    wanted = jnp.zeros((n, lanes), WIDE)
    for g in range(groups):
        listing = chosen_ref[:, g, :]
        hit = (listing >= me * per_block) & (listing < (me + 1) * per_block)
        inner = jnp.where(hit, (listing - me * per_block).astype(WIDE), 0.0)
        wanted = jnp.where(lane_group == g, jnp.sum(inner, -1, keepdims=True), wanted)
    table[...] = wanted
    want = [table[pl.ds(to[s], 1), :] for s in range(n)]

    keys = k_ref[...].astype(WIDE)
    values = v_ref[...].astype(WIDE)

    def summary_of(array):
        row = lax.broadcasted_iota(jnp.int32, (pad, lanes), 0)
        result = jnp.zeros((pad, lanes), WIDE)
        for j in range(per_summary):
            mean = jnp.sum(array[j * CMP : (j + 1) * CMP], 0, keepdims=True) / CMP
            result = jnp.where(row == j, mean, result)
        return result

    def block_of(array, row):
        result = array[:BLK]
        for b in range(1, per_block):
            result = jnp.where(row == b, array[b * BLK : (b + 1) * BLK], result)
        return result.astype(LOW)

    sum_out[...] = jnp.concatenate([summary_of(keys), summary_of(values)], 0).astype(LOW)
    sum_in[0] = sum_out[...]
    for s in range(n):
        target = blk_in if s == 0 else blk_out
        target[s, :BLK] = block_of(keys, want[s])
        target[s, BLK : 2 * BLK] = block_of(values, want[s])

    pl.semaphore_wait(barrier, n - 1 + tps - 1)
    blk = [
        copy(blk_out.at[s], blk_in.at[s], blk_send.at[s], blk_recv.at[s], kv=to[s]) for s in range(1, n)
    ]
    summed_in = [
        copy(sum_out, sum_in.at[s], sum_send.at[s], sum_recv.at[s], kv=to[s]) for s in range(1, n)
    ]
    for c in summed_in:
        c.start()
    each(blk, later, lambda c: c.start())
    hid = [
        copy(hidden_of(to[s]), hid_in.at[s, part_rows], hid_send.at[s], hid_recv.at[s], kv=to[s])
        for s in range(1, n)
    ]
    for c in hid:
        c.start()

    for c in loads[3:]:
        c.wait()
    columns = jnp.concatenate([log_ref[0], log_ref[1], gate_ref[0], gate_ref[1]], 0).T

    def column(kind, branch, h, count):
        at = (2 * kind + branch) * heads + h
        return columns[:count, at : at + 1]

    def head_stats(branch, h, count):
        at = slice(h * DH, (h + 1) * DH)
        gated = column(1, branch, h, count) * cot_ref[:count, at].astype(WIDE)
        delta = jnp.sum(gated * out_ref[branch, :count, at].astype(WIDE), -1, keepdims=True)
        return gated.astype(LOW), delta, column(0, branch, h, count), q_ref[:count, at]

    def stats(branch, g, count):
        found = [head_stats(branch, g * group_heads + r, count) for r in range(group_heads)]
        return [jnp.concatenate(piece, 0) for piece in zip(*found)]

    prepared = [(stats(0, g, rows), stats(1, g, qrows)) for g in range(groups)]

    def owner_of(shape, per_slot):
        column_at = lax.broadcasted_iota(jnp.int32, shape, 1)
        slot = column_at // per_slot
        owner = 2 * lax.rem(place + half - slot // 2, half) + lax.rem(side + slot % 2, 2)
        return owner, column_at % per_slot

    shape0 = (group_heads * rows, n * pad)
    owner0, inner0 = owner_of(shape0, pad)
    time0 = me * rows + lax.broadcasted_iota(jnp.int32, shape0, 0) % rows
    seen0 = (inner0 < per_summary) & ((owner0 * per_summary + inner0 + 1) * CMP - 1 <= time0)
    shape1 = (group_heads * qrows, n * BLK)
    owner1, inner1 = owner_of(shape1, BLK)
    time1 = lax.broadcasted_iota(jnp.int32, shape1, 0) % qrows

    def branch(query, key, value, seen, low, delta, log):
        probs = jnp.where(seen, jnp.exp(dot(query, key, NT) * scale - log), 0.0)
        score = (probs * (dot(low, value, NT) - delta)).astype(LOW)
        return probs.astype(LOW), score

    for c in summed_in:
        c.wait_recv()
    all_sums = sum_in[...].astype(WIDE)
    all_sum_keys = all_sums[:, :pad].reshape(n * pad, lanes).astype(LOW)
    all_sum_values = all_sums[:, pad:].reshape(n * pad, lanes).astype(LOW)

    def wide_of(parts):
        return jnp.concatenate(parts, 1)

    grad0, key0, value0 = [], [], []
    for g in range(groups):
        at = slice(g * DH, (g + 1) * DH)
        low0, delta0, log0, query0 = prepared[g][0]
        probs0, score0 = branch(query0, all_sum_keys[:, at], all_sum_values[:, at], seen0, low0, delta0, log0)
        grad0.append(dot(score0, all_sum_keys[:, at], NN) * scale)
        for r in range(group_heads):
            h = slice((g * group_heads + r) * DH, (g * group_heads + r + 1) * DH)
            gq_ref[qrows:, h] = grad0[g][r * rows + qrows : (r + 1) * rows]
        key0.append((score0, query0))
        value0.append((probs0, low0))
    direct = [s for s in range(1, n) if s % 2 == 0 or s == 1]
    pieces = (slice(qrows, rows), slice(0, qrows))
    qb = [
        {
            s: copy(qb_out.at[piece], qb_in.at[s, piece], qb_send.at[i, s], qb_recv.at[i, s], kv=to[s])
            for s in direct
        }
        for i, piece in enumerate(pieces)
    ]
    passed = [
        {
            s: copy(
                qb_in.at[s, piece], qb_in.at[s + 1, piece],
                pass_send.at[i, s], pass_recv.at[i, s], kv=to[1],
            )
            for s in range(2, n, 2)
        }
        for i, piece in enumerate(pieces)
    ]
    qb_out[qrows:] = gq_ref[qrows:].astype(LOW)
    for s in reversed(direct):
        qb[0][s].start()
    key0 = wide_of([dot(score, query, TN) for score, query in key0]) * scale
    value0 = wide_of([dot(probs, low, TN) for probs, low in value0])

    each(blk, earlier, lambda c: c.wait_recv())
    all_keys = blk_in[:, :BLK].reshape(n * BLK, lanes)
    all_values = blk_in[:, BLK:].reshape(n * BLK, lanes)
    key1, value1 = [], []
    for g in range(groups):
        at = slice(g * DH, (g + 1) * DH)
        low1, delta1, log1, query1 = prepared[g][1]
        own_block = want[0][:, g * DH : g * DH + 1]
        first = own_block * BLK + inner1.astype(WIDE) <= time1.astype(WIDE)
        seen1 = (owner1 < me) | ((owner1 == me) & first)
        probs1, score1 = branch(query1, all_keys[:, at], all_values[:, at], seen1, low1, delta1, log1)
        grad1 = dot(score1, all_keys[:, at], NN) * scale
        for r in range(group_heads):
            h = slice((g * group_heads + r) * DH, (g * group_heads + r + 1) * DH)
            gq_ref[:qrows, h] = grad0[g][r * rows : r * rows + qrows] + grad1[r * qrows : (r + 1) * qrows]
        key1.append((score1, query1))
        value1.append((probs1, low1))
    qb_out[:qrows] = gq_ref[:qrows].astype(LOW)
    for s in reversed(direct):
        qb[1][s].start()
    key1 = wide_of([dot(score, query, TN) for score, query in key1]) * scale
    value1 = wide_of([dot(probs, low, TN) for probs, low in value1])
    for s in range(1, n):
        grd_out[s, :BLK] = key1[s * BLK : (s + 1) * BLK].astype(LOW)
        grd_out[s, BLK : 2 * BLK] = value1[s * BLK : (s + 1) * BLK].astype(LOW)
        both = [key0[s * pad : (s + 1) * pad], value0[s * pad : (s + 1) * pad]]
        grd_out[s, 2 * BLK :] = jnp.concatenate(both, 0).astype(LOW)
    grd = [
        copy(grd_out.at[s], grd_in.at[s], grd_send.at[s], grd_recv.at[s], kv=come[s])
        for s in range(1, n)
    ]
    each(grd, earlier, lambda c: c.start())

    own_hidden.wait()
    for c in hid:
        c.wait_recv()
    mine = hid_in.at[:, part_rows]
    share = [
        copy(mine, mine, share_send.at[u], share_recv.at[u], tp=tp_to[u]) for u in range(1, tps)
    ]
    for c in share:
        c.start()

    for i in range(len(pieces)):
        for s in range(2, n, 2):
            qb[i][s].wait_recv()
            passed[i][s].start()

    for u in range(1, tps):
        other = lax.rem(my_tp + tps - u, tps)
        arrived = hid_in.at[:, pl.ds(pl.multiple_of(other * part, part), part)]
        copy(mine, arrived, share_send.at[u], share_recv.at[u], tp=tp_to[u]).wait_recv()
    for s in range(n):
        hid_t[s] = hid_in[s].T
    total = dot(hid_t[0], qb_out[...], NN)
    for s in range(2, n, 2):
        total = total + dot(hid_t[s], qb_in[s], NN)
    for i in range(len(pieces)):
        qb[i][1].wait_recv()
    total = total + dot(hid_t[1], qb_in[1], NN)

    each(grd, later, lambda c: c.wait_recv())
    for block_part, sum_part, own_block, own_sum, result in (
        (0, 0, key1, key0, gk_ref),
        (BLK, pad, value1, value0, gv_ref),
    ):
        here = [own_block[:BLK]]
        summed = own_sum[:pad]
        for s in range(1, n):
            here.append(grd_in[s, block_part : block_part + BLK].astype(WIDE))
            summed = summed + grd_in[s, 2 * BLK :].astype(WIDE)[sum_part : sum_part + pad]
        for b in range(per_block):
            block = jnp.zeros((BLK, lanes), WIDE)
            for s in range(n):
                block = block + jnp.where(want[s] == b, here[s], 0.0)
            for j in range(BLK // CMP):
                at = b * BLK + j * CMP
                term = summed[at // CMP : at // CMP + 1] / CMP
                result[at : at + CMP] = block[j * CMP : (j + 1) * CMP] + term

    for s in range(2, n, 2):
        for i in range(len(pieces)):
            passed[i][s].wait_recv()
        total = total + dot(hid_t[s + 1], qb_in[s + 1], NN)
    gw_ref[...] = total
    for c in summed_in + hid + share:
        c.wait_send()
    for i in range(len(pieces)):
        for c in list(qb[i].values()) + list(passed[i].values()):
            c.wait_send()
    each(blk, later, lambda c: c.wait_send())
    each(grd, earlier, lambda c: c.wait_send())


def fused(n, tps, queries, keys, values, hidden, log_sums, gates, branch_out, cotangent, chosen):
    rows, width = queries.shape
    lanes = keys.shape[1]
    cols = hidden.shape[1] // n
    pad = -(-(rows // CMP) // 8) * 8
    groups, nsel = chosen.shape[1:]
    heads = log_sums.shape[2]
    vmem = pl.BlockSpec(memory_space=pltpu.VMEM)
    sems = pltpu.SemaphoreType.DMA((n,))
    two_sems = pltpu.SemaphoreType.DMA((2, n))
    tp_sems = pltpu.SemaphoreType.DMA((tps,))
    return pl.pallas_call(
        functools.partial(fused_kernel, n, tps),
        out_shape=(
            jax.ShapeDtypeStruct((rows, width), WIDE),
            jax.ShapeDtypeStruct((rows, lanes), WIDE),
            jax.ShapeDtypeStruct((rows, lanes), WIDE),
            jax.ShapeDtypeStruct((cols, width), WIDE),
        ),
        in_specs=[pl.BlockSpec(memory_space=pl.ANY)] * 9,
        out_specs=(vmem,) * 4,
        scratch_shapes=[
            pltpu.VMEM((rows, lanes), LOW),
            pltpu.VMEM((rows, lanes), LOW),
            pltpu.VMEM((n, groups, nsel), jnp.int32),
            pltpu.VMEM((rows, width), LOW),
            pltpu.VMEM((rows, width), LOW),
            pltpu.VMEM((2, heads, rows), WIDE),
            pltpu.VMEM((2, rows, width), LOW),
            pltpu.VMEM((2, heads, rows), WIDE),
            pltpu.VMEM((n, lanes), WIDE),
            pltpu.VMEM((2 * pad, lanes), LOW),
            pltpu.VMEM((n, 2 * pad, lanes), LOW),
            pltpu.VMEM((n, 2 * BLK, lanes), LOW),
            pltpu.VMEM((n, 2 * BLK, lanes), LOW),
            pltpu.VMEM((n, 2 * BLK + 2 * pad, lanes), LOW),
            pltpu.VMEM((n, 2 * BLK + 2 * pad, lanes), LOW),
            pltpu.VMEM((rows, width), LOW),
            pltpu.VMEM((n, rows, width), LOW),
            pltpu.VMEM((n, rows, cols), LOW),
            pltpu.VMEM((n, cols, rows), LOW),
            sems, sems, sems, sems, sems, sems, two_sems, two_sems, sems, sems, two_sems, two_sems,
            tp_sems, tp_sems,
            pltpu.SemaphoreType.DMA,
            pltpu.SemaphoreType.DMA((8,)),
        ],
        compiler_params=pltpu.CompilerParams(collective_id=0, has_side_effects=True),
    )(
        queries, keys, values, hidden, jnp.swapaxes(log_sums, 1, 2), jnp.swapaxes(gates, 1, 2),
        branch_out, cotangent, chosen,
    )


def fits(n, tps, hidden, chosen):
    whole = (hidden.shape[1] // n) % 128 == 0 and (hidden.shape[0] // tps) % 16 == 0
    return chosen.shape[0] <= TOPN and n % 2 == 0 and whole


def solution(mesh):

    n, tps = mesh.shape["kv"], mesh.shape["tp"]

    def body(*args):
        return fused(n, tps, *args) if fits(n, tps, args[3], args[8]) else shards(*args)

    return jax.shard_map(
        body,
        mesh=mesh,
        in_specs=(
            P("kv", "tp"),
            P("kv", "tp"),
            P("kv", "tp"),
            P("kv", None),
            P(None, "kv", "tp"),
            P(None, "kv", "tp"),
            P(None, "kv", "tp"),
            P("kv", "tp"),
            P(None, "tp", None),
        ),
        out_specs=(P("kv", "tp"), P("kv", "tp"), P("kv", "tp"), P("kv", "tp")),
        check_vma=False,
    )
```

```python
import functools

import jax
import jax.numpy as jnp
from jax import lax
from jax.experimental import pallas as pl
from jax.experimental.pallas import tpu as pltpu
from jax.sharding import PartitionSpec as P

DH = 64
BLK = 32
TOPN = 12
SUB = 4
CMP = 32


def branch_grads(query_rows, key_rows, value_rows, seen, log_rows, delta_rows, cot_rows, scale):
    wide = jnp.float32
    scores = jnp.einsum("tgre,gme->grtm", query_rows, key_rows, preferred_element_type=wide) * scale
    log_here = jnp.transpose(log_rows, (1, 2, 0))[..., None]
    delta_here = jnp.transpose(delta_rows, (1, 2, 0))[..., None]
    probs = jnp.where(seen[:, None], jnp.exp(scores - log_here), 0.0)
    probs_low = probs.astype(jnp.bfloat16)
    value_grad = jnp.einsum("grtm,tgre->gme", probs_low, cot_rows, preferred_element_type=wide)
    prob_grad = jnp.einsum("tgre,gme->grtm", cot_rows, value_rows, preferred_element_type=wide)
    score_low = (probs * (prob_grad - delta_here)).astype(jnp.bfloat16)
    query_grad = (
        jnp.einsum("grtm,gme->tgre", score_low, key_rows, preferred_element_type=wide) * scale
    )
    key_grad = (
        jnp.einsum("grtm,tgre->gme", score_low, query_rows, preferred_element_type=wide) * scale
    )
    return (query_grad, key_grad, value_grad)


def shards(queries, keys, values, hidden, log_sums, gates, branch_out, cotangent, chosen):
    wide = jnp.float32
    rows_here = queries.shape[0]
    heads = queries.shape[1] // DH
    groups = keys.shape[1] // DH
    group_heads = heads // groups
    per_block = rows_here // BLK
    per_summary = rows_here // CMP
    blocks_all = chosen.shape[0]
    nsel = chosen.shape[2]
    qrows = rows_here // SUB
    scale = DH ** (-0.5)
    grads_each = jax.vmap(branch_grads, in_axes=(0, 0, 0, 0, 0, 0, 0, None))
    place = lax.axis_index("kv")
    position = place * rows_here + jnp.arange(rows_here, dtype=jnp.int32)
    gated = gates[..., None] * cotangent.reshape(rows_here, heads, DH).astype(wide)[None]
    delta_all = jnp.sum(gated * branch_out.reshape(2, rows_here, heads, DH).astype(wide), -1)
    delta_all = delta_all.reshape(2, rows_here, groups, group_heads)
    gated_low = gated.astype(jnp.bfloat16).reshape(2, rows_here, groups, group_heads, DH)
    log_all = log_sums.reshape(2, rows_here, groups, group_heads)
    query_all = queries.reshape(rows_here, groups, group_heads, DH)
    pairs = jnp.concatenate(
        [keys.reshape(rows_here, groups, DH), values.reshape(rows_here, groups, DH)], -1
    )
    means = jnp.mean(pairs.reshape(per_summary, CMP, groups, 2 * DH).astype(wide), 1).astype(
        jnp.bfloat16
    )
    summaries = lax.all_gather(means, "kv", axis=0, tiled=True)
    summary_count = summaries.shape[0]
    sum_keys = jnp.transpose(summaries[..., :DH], (1, 0, 2))
    sum_values = jnp.transpose(summaries[..., DH:], (1, 0, 2))
    summary_end = jnp.arange(summary_count, dtype=jnp.int32) * CMP + CMP - 1
    summary_seen = (summary_end[None, :] <= position[:, None])[None]
    query_sum, key_sum, value_sum = branch_grads(
        query_all, sum_keys, sum_values, summary_seen, log_all[0], delta_all[0], gated_low[0], scale
    )
    summary_term = jnp.transpose(jnp.concatenate([key_sum, value_sum], -1), (1, 0, 2))
    listing = lax.dynamic_index_in_dim(chosen, place, 0, keepdims=False)
    live = listing >= 0
    safe = jnp.maximum(listing, 0)
    owner = safe // per_block
    group_index = jnp.arange(groups, dtype=jnp.int32)
    hits = (chosen >= 0) & (chosen // per_block == place)
    wanted = jnp.sum(jnp.where(hits, chosen % per_block, 0), -1)
    asked = jnp.any(hits, -1)
    row_target = safe[..., None] * BLK + jnp.arange(BLK, dtype=jnp.int32)
    pair_blocks = pairs.reshape(per_block, BLK, groups, 2 * DH)
    outbound = pair_blocks[wanted, :, group_index[None, :], :]
    arrived = lax.all_to_all(outbound, "kv", split_axis=0, concat_axis=0, tiled=True)
    picked = arrived[owner, group_index[:, None]]

    def by_sub(array):
        rest = array.shape[3:]
        moved = array.reshape((groups, SUB, TOPN * BLK) + rest)
        return jnp.swapaxes(moved, 0, 1)

    picked_sub = by_sub(picked)
    picked_keys = picked_sub[..., :DH]
    picked_values = picked_sub[..., DH:]
    live_rows = by_sub(jnp.broadcast_to(live[..., None], (groups, nsel, BLK)))
    key_position = by_sub(row_target)
    sub_position = position.reshape(SUB, qrows)
    block_seen = live_rows[:, :, None, :] & (
        key_position[:, :, None, :] <= sub_position[:, None, :, None]
    )
    query_sel, key_sel, value_sel = grads_each(
        query_all.reshape(SUB, qrows, groups, group_heads, DH),
        picked_keys,
        picked_values,
        block_seen,
        log_all[1].reshape(SUB, qrows, groups, group_heads),
        delta_all[1].reshape(SUB, qrows, groups, group_heads),
        gated_low[1].reshape(SUB, qrows, groups, group_heads, DH),
        scale,
    )
    query_sel = query_sel.reshape(rows_here, groups, group_heads, DH)
    key_sel = jnp.swapaxes(key_sel, 0, 1).reshape(groups, nsel, BLK, DH)
    value_sel = jnp.swapaxes(value_sel, 0, 1).reshape(groups, nsel, BLK, DH)
    slot_grads = jnp.concatenate([key_sel, value_sel], -1)
    slot_grads = slot_grads * live[..., None, None].astype(wide)
    outgoing = (
        jnp.zeros((blocks_all, groups, BLK, 2 * DH), wide)
        .at[owner, group_index[:, None]]
        .add(slot_grads)
    )
    summary_out = jnp.transpose(
        summary_term.reshape(blocks_all, per_summary, groups, 2 * DH), (0, 2, 1, 3)
    )
    both_out = jnp.concatenate([outgoing, summary_out], 2)
    both_in = lax.all_to_all(
        both_out.astype(jnp.bfloat16), "kv", split_axis=0, concat_axis=0, tiled=True
    ).astype(both_out.dtype)
    incoming = both_in[:, :, :BLK]
    summary_mine = jnp.transpose(jnp.sum(both_in[:, :, BLK:], 0), (1, 0, 2))
    selector = (
        (wanted[..., None] == jnp.arange(per_block, dtype=jnp.int32)) & asked[..., None]
    ).astype(wide)
    block_sums = jnp.einsum("rgb,rgkc->bkgc", selector, incoming, precision=lax.Precision.HIGHEST)
    pair_grads = (
        block_sums.reshape(rows_here, groups, 2 * DH) + jnp.repeat(summary_mine, CMP, axis=0) / CMP
    )
    grad_queries = (query_sum + query_sel).reshape(rows_here, heads * DH)
    query_low = grad_queries.astype(jnp.bfloat16)
    grad_weight = lax.psum_scatter(
        lax.dot_general(
            hidden, query_low, (((0,), (0,)), ((), ())), preferred_element_type=jnp.float32
        ),
        "kv",
        scatter_dimension=0,
        tiled=True,
    )
    grad_keys = pair_grads[..., :DH].reshape(rows_here, groups * DH)
    grad_values = pair_grads[..., DH:].reshape(rows_here, groups * DH)
    return (grad_queries, grad_keys, grad_values, grad_weight)


WIDE = jnp.float32
LOW = jnp.bfloat16
NT = (((1,), (1,)), ((), ()))
TN = (((0,), (0,)), ((), ()))
NN = (((1,), (0,)), ((), ()))


def dot(a, b, dims):
    return lax.dot_general(a, b, dims, preferred_element_type=WIDE)


def fused_kernel(
    n, tps, q_hbm, k_hbm, v_hbm, hid_ref, log_hbm, gate_hbm, out_hbm, cot_hbm, chosen_hbm,
    gq_ref, gk_ref, gv_ref, gw_ref,
    k_ref, v_ref, chosen_ref, q_ref, cot_ref, gate_ref, out_ref, log_ref,
    table, sum_out, sum_in, blk_out, blk_in, grd_out, grd_in, qb_out, qb_in, hid_in, hid_t,
    sum_send, sum_recv, blk_send, blk_recv, hid_send, hid_recv, qb_send, qb_recv,
    grd_send, grd_recv, pass_send, pass_recv, share_send, share_recv, own_sem, load_sem,
):
    rows, width = q_ref.shape
    heads = width // DH
    lanes = k_ref.shape[1]
    groups = lanes // DH
    group_heads = heads // groups
    per_block = rows // BLK
    per_summary = rows // CMP
    pad = sum_in.shape[1] // 2
    qrows = rows // SUB
    cols = hid_in.shape[2]
    part = rows // tps
    scale = DH ** (-0.5)
    me = lax.axis_index("kv")
    my_tp = lax.axis_index("tp")
    half = n // 2
    place, side = me // 2, me % 2
    to = [2 * lax.rem(place + s // 2, half) + lax.rem(side + s % 2, 2) for s in range(n)]
    come = [2 * lax.rem(place + half - s // 2, half) + lax.rem(side + s % 2, 2) for s in range(n)]
    mesh_id = pl.DeviceIdType.MESH

    def copy(src, dst, send, recv, **peer):
        return pltpu.make_async_remote_copy(
            src_ref=src, dst_ref=dst, send_sem=send, recv_sem=recv,
            device_id=peer, device_id_type=mesh_id,
        )

    pairs = (
        (k_hbm, k_ref), (v_hbm, v_ref), (chosen_hbm, chosen_ref), (q_hbm, q_ref),
        (cot_hbm, cot_ref), (gate_hbm, gate_ref), (out_hbm, out_ref), (log_hbm, log_ref),
    )
    loads = [pltpu.make_async_copy(*pair, load_sem.at[i]) for i, pair in enumerate(pairs)]
    barrier = pltpu.get_barrier_semaphore()
    for s in range(n - 1, 0, -1):
        pl.semaphore_signal(barrier, inc=1, device_id={"kv": to[s]}, device_id_type=mesh_id)
    tp_to = [lax.rem(my_tp + u, tps) for u in range(tps)]
    for u in range(1, tps):
        pl.semaphore_signal(barrier, inc=1, device_id={"tp": tp_to[u]}, device_id_type=mesh_id)

    for c in loads:
        c.start()
    later = [to[s] > me for s in range(n)]
    earlier = [come[s] < me for s in range(n)]

    def each(copies, conditions, act):
        for c, condition in zip(copies, conditions[1:]):
            pl.when(condition)(functools.partial(act, c))

    for s in range(1, n):

        @pl.when(jnp.logical_not(earlier[s]))
        def _():
            blk_in[s] = jnp.zeros(blk_in.shape[1:], LOW)

        @pl.when(jnp.logical_not(later[s]))
        def _():
            grd_in[s] = jnp.zeros(grd_in.shape[1:], LOW)

    part_rows = pl.ds(pl.multiple_of(my_tp * part, part), part)

    def hidden_of(peer):
        return hid_ref.at[part_rows, pl.ds(pl.multiple_of(peer * cols, cols), cols)]

    own_hidden = pltpu.make_async_copy(hidden_of(me), hid_in.at[0, part_rows], own_sem)
    own_hidden.start()

    for c in loads[:3]:
        c.wait()
    lane_group = lax.broadcasted_iota(jnp.int32, (n, lanes), 1) // DH
    wanted = jnp.zeros((n, lanes), WIDE)
    for g in range(groups):
        listing = chosen_ref[:, g, :]
        hit = (listing >= me * per_block) & (listing < (me + 1) * per_block)
        inner = jnp.where(hit, (listing - me * per_block).astype(WIDE), 0.0)
        wanted = jnp.where(lane_group == g, jnp.sum(inner, -1, keepdims=True), wanted)
    table[...] = wanted
    want = [table[pl.ds(to[s], 1), :] for s in range(n)]

    keys = k_ref[...].astype(WIDE)
    values = v_ref[...].astype(WIDE)

    def summary_of(array):
        row = lax.broadcasted_iota(jnp.int32, (pad, lanes), 0)
        result = jnp.zeros((pad, lanes), WIDE)
        for j in range(per_summary):
            mean = jnp.sum(array[j * CMP : (j + 1) * CMP], 0, keepdims=True) / CMP
            result = jnp.where(row == j, mean, result)
        return result

    def block_of(array, row):
        result = array[:BLK]
        for b in range(1, per_block):
            result = jnp.where(row == b, array[b * BLK : (b + 1) * BLK], result)
        return result.astype(LOW)

    sum_out[...] = jnp.concatenate([summary_of(keys), summary_of(values)], 0).astype(LOW)
    sum_in[0] = sum_out[...]
    for s in range(n):
        target = blk_in if s == 0 else blk_out
        target[s, :BLK] = block_of(keys, want[s])
        target[s, BLK : 2 * BLK] = block_of(values, want[s])

    pl.semaphore_wait(barrier, n - 1 + tps - 1)
    blk = [
        copy(blk_out.at[s], blk_in.at[s], blk_send.at[s], blk_recv.at[s], kv=to[s]) for s in range(1, n)
    ]
    summed_in = [
        copy(sum_out, sum_in.at[s], sum_send.at[s], sum_recv.at[s], kv=to[s]) for s in range(1, n)
    ]
    for c in summed_in:
        c.start()
    each(blk, later, lambda c: c.start())
    hid = [
        copy(hidden_of(to[s]), hid_in.at[s, part_rows], hid_send.at[s], hid_recv.at[s], kv=to[s])
        for s in range(1, n)
    ]
    for c in hid:
        c.start()

    for c in loads[3:]:
        c.wait()
    columns = jnp.concatenate([log_ref[0], log_ref[1], gate_ref[0], gate_ref[1]], 0).T

    def column(kind, branch, h, count):
        at = (2 * kind + branch) * heads + h
        return columns[:count, at : at + 1]

    def head_stats(branch, h, count):
        at = slice(h * DH, (h + 1) * DH)
        gated = column(1, branch, h, count) * cot_ref[:count, at].astype(WIDE)
        delta = jnp.sum(gated * out_ref[branch, :count, at].astype(WIDE), -1, keepdims=True)
        return gated.astype(LOW), delta, column(0, branch, h, count), q_ref[:count, at]

    def stats(branch, g, count):
        found = [head_stats(branch, g * group_heads + r, count) for r in range(group_heads)]
        return [jnp.concatenate(piece, 0) for piece in zip(*found)]

    prepared = [(stats(0, g, rows), stats(1, g, qrows)) for g in range(groups)]

    def owner_of(shape, per_slot):
        column_at = lax.broadcasted_iota(jnp.int32, shape, 1)
        slot = column_at // per_slot
        owner = 2 * lax.rem(place + half - slot // 2, half) + lax.rem(side + slot % 2, 2)
        return owner, column_at % per_slot

    shape0 = (group_heads * rows, n * pad)
    owner0, inner0 = owner_of(shape0, pad)
    time0 = me * rows + lax.broadcasted_iota(jnp.int32, shape0, 0) % rows
    seen0 = (inner0 < per_summary) & ((owner0 * per_summary + inner0 + 1) * CMP - 1 <= time0)
    shape1 = (group_heads * qrows, n * BLK)
    owner1, inner1 = owner_of(shape1, BLK)
    time1 = lax.broadcasted_iota(jnp.int32, shape1, 0) % qrows

    def branch(query, key, value, seen, low, delta, log):
        probs = jnp.where(seen, jnp.exp(dot(query, key, NT) * scale - log), 0.0)
        score = (probs * (dot(low, value, NT) - delta)).astype(LOW)
        return probs.astype(LOW), score

    for c in summed_in:
        c.wait_recv()
    all_sums = sum_in[...].astype(WIDE)
    all_sum_keys = all_sums[:, :pad].reshape(n * pad, lanes).astype(LOW)
    all_sum_values = all_sums[:, pad:].reshape(n * pad, lanes).astype(LOW)

    def wide_of(parts):
        return jnp.concatenate(parts, 1)

    grad0, key0, value0 = [], [], []
    for g in range(groups):
        at = slice(g * DH, (g + 1) * DH)
        low0, delta0, log0, query0 = prepared[g][0]
        probs0, score0 = branch(query0, all_sum_keys[:, at], all_sum_values[:, at], seen0, low0, delta0, log0)
        grad0.append(dot(score0, all_sum_keys[:, at], NN) * scale)
        for r in range(group_heads):
            h = slice((g * group_heads + r) * DH, (g * group_heads + r + 1) * DH)
            gq_ref[qrows:, h] = grad0[g][r * rows + qrows : (r + 1) * rows]
        key0.append((score0, query0))
        value0.append((probs0, low0))
    direct = [s for s in range(1, n) if s % 2 == 0 or s == 1]
    pieces = (slice(qrows, rows), slice(0, qrows))
    qb = [
        {
            s: copy(qb_out.at[piece], qb_in.at[s, piece], qb_send.at[i, s], qb_recv.at[i, s], kv=to[s])
            for s in direct
        }
        for i, piece in enumerate(pieces)
    ]
    passed = [
        {
            s: copy(
                qb_in.at[s, piece], qb_in.at[s + 1, piece],
                pass_send.at[i, s], pass_recv.at[i, s], kv=to[1],
            )
            for s in range(2, n, 2)
        }
        for i, piece in enumerate(pieces)
    ]
    qb_out[qrows:] = gq_ref[qrows:].astype(LOW)
    for s in reversed(direct):
        qb[0][s].start()
    key0 = wide_of([dot(score, query, TN) for score, query in key0]) * scale
    value0 = wide_of([dot(probs, low, TN) for probs, low in value0])

    each(blk, earlier, lambda c: c.wait_recv())
    all_keys = blk_in[:, :BLK].reshape(n * BLK, lanes)
    all_values = blk_in[:, BLK:].reshape(n * BLK, lanes)
    key1, value1 = [], []
    for g in range(groups):
        at = slice(g * DH, (g + 1) * DH)
        low1, delta1, log1, query1 = prepared[g][1]
        own_block = want[0][:, g * DH : g * DH + 1]
        first = own_block * BLK + inner1.astype(WIDE) <= time1.astype(WIDE)
        seen1 = (owner1 < me) | ((owner1 == me) & first)
        probs1, score1 = branch(query1, all_keys[:, at], all_values[:, at], seen1, low1, delta1, log1)
        grad1 = dot(score1, all_keys[:, at], NN) * scale
        for r in range(group_heads):
            h = slice((g * group_heads + r) * DH, (g * group_heads + r + 1) * DH)
            gq_ref[:qrows, h] = grad0[g][r * rows : r * rows + qrows] + grad1[r * qrows : (r + 1) * qrows]
        key1.append((score1, query1))
        value1.append((probs1, low1))
    qb_out[:qrows] = gq_ref[:qrows].astype(LOW)
    for s in reversed(direct):
        qb[1][s].start()
    key1 = wide_of([dot(score, query, TN) for score, query in key1]) * scale
    value1 = wide_of([dot(probs, low, TN) for probs, low in value1])
    for s in range(1, n):
        grd_out[s, :BLK] = key1[s * BLK : (s + 1) * BLK].astype(LOW)
        grd_out[s, BLK : 2 * BLK] = value1[s * BLK : (s + 1) * BLK].astype(LOW)
        both = [key0[s * pad : (s + 1) * pad], value0[s * pad : (s + 1) * pad]]
        grd_out[s, 2 * BLK :] = jnp.concatenate(both, 0).astype(LOW)
    grd = [
        copy(grd_out.at[s], grd_in.at[s], grd_send.at[s], grd_recv.at[s], kv=come[s])
        for s in range(1, n)
    ]
    each(grd, earlier, lambda c: c.start())

    own_hidden.wait()
    for c in hid:
        c.wait_recv()
    mine = hid_in.at[:, part_rows]
    share = [
        copy(mine, mine, share_send.at[u], share_recv.at[u], tp=tp_to[u]) for u in range(1, tps)
    ]
    for c in share:
        c.start()

    for i in range(len(pieces)):
        for s in range(2, n, 2):
            qb[i][s].wait_recv()
            passed[i][s].start()

    for u in range(1, tps):
        other = lax.rem(my_tp + tps - u, tps)
        arrived = hid_in.at[:, pl.ds(pl.multiple_of(other * part, part), part)]
        copy(mine, arrived, share_send.at[u], share_recv.at[u], tp=tp_to[u]).wait_recv()
    for s in range(n):
        hid_t[s] = hid_in[s].T
    total = dot(hid_t[0], qb_out[...], NN)
    for s in range(2, n, 2):
        total = total + dot(hid_t[s], qb_in[s], NN)
    for i in range(len(pieces)):
        qb[i][1].wait_recv()
    total = total + dot(hid_t[1], qb_in[1], NN)

    each(grd, later, lambda c: c.wait_recv())
    for block_part, sum_part, own_block, own_sum, result in (
        (0, 0, key1, key0, gk_ref),
        (BLK, pad, value1, value0, gv_ref),
    ):
        here = [own_block[:BLK]]
        summed = own_sum[:pad]
        for s in range(1, n):
            here.append(grd_in[s, block_part : block_part + BLK].astype(WIDE))
            summed = summed + grd_in[s, 2 * BLK :].astype(WIDE)[sum_part : sum_part + pad]
        for b in range(per_block):
            block = jnp.zeros((BLK, lanes), WIDE)
            for s in range(n):
                block = block + jnp.where(want[s] == b, here[s], 0.0)
            for j in range(BLK // CMP):
                at = b * BLK + j * CMP
                term = summed[at // CMP : at // CMP + 1] / CMP
                result[at : at + CMP] = block[j * CMP : (j + 1) * CMP] + term

    for s in range(2, n, 2):
        for i in range(len(pieces)):
            passed[i][s].wait_recv()
        total = total + dot(hid_t[s + 1], qb_in[s + 1], NN)
    gw_ref[...] = total
    for c in summed_in + hid + share:
        c.wait_send()
    for i in range(len(pieces)):
        for c in list(qb[i].values()) + list(passed[i].values()):
            c.wait_send()
    each(blk, later, lambda c: c.wait_send())
    each(grd, earlier, lambda c: c.wait_send())


def place_kernel(*refs):
    count = len(refs) // 2
    for source, target in zip(refs[:count], refs[count:]):
        target[...] = source[...]


def fused(n, tps, queries, keys, values, hidden, log_sums, gates, branch_out, cotangent, chosen):
    rows, width = queries.shape
    lanes = keys.shape[1]
    cols = hidden.shape[1] // n
    pad = -(-(rows // CMP) // 8) * 8
    groups, nsel = chosen.shape[1:]
    heads = log_sums.shape[2]
    vmem = pl.BlockSpec(memory_space=pltpu.VMEM)
    shapes = ((rows, width), (rows, lanes), (rows, lanes), (cols, width))
    sems = pltpu.SemaphoreType.DMA((n,))
    two_sems = pltpu.SemaphoreType.DMA((2, n))
    tp_sems = pltpu.SemaphoreType.DMA((tps,))
    results = pl.pallas_call(
        functools.partial(fused_kernel, n, tps),
        out_shape=tuple(pltpu.VMEM(shape, WIDE) for shape in shapes),
        in_specs=[pl.BlockSpec(memory_space=pl.ANY)] * 9,
        out_specs=(vmem,) * 4,
        scratch_shapes=[
            pltpu.VMEM((rows, lanes), LOW),
            pltpu.VMEM((rows, lanes), LOW),
            pltpu.VMEM((n, groups, nsel), jnp.int32),
            pltpu.VMEM((rows, width), LOW),
            pltpu.VMEM((rows, width), LOW),
            pltpu.VMEM((2, heads, rows), WIDE),
            pltpu.VMEM((2, rows, width), LOW),
            pltpu.VMEM((2, heads, rows), WIDE),
            pltpu.VMEM((n, lanes), WIDE),
            pltpu.VMEM((2 * pad, lanes), LOW),
            pltpu.VMEM((n, 2 * pad, lanes), LOW),
            pltpu.VMEM((n, 2 * BLK, lanes), LOW),
            pltpu.VMEM((n, 2 * BLK, lanes), LOW),
            pltpu.VMEM((n, 2 * BLK + 2 * pad, lanes), LOW),
            pltpu.VMEM((n, 2 * BLK + 2 * pad, lanes), LOW),
            pltpu.VMEM((rows, width), LOW),
            pltpu.VMEM((n, rows, width), LOW),
            pltpu.VMEM((n, rows, cols), LOW),
            pltpu.VMEM((n, cols, rows), LOW),
            sems, sems, sems, sems, sems, sems, two_sems, two_sems, sems, sems, two_sems, two_sems,
            tp_sems, tp_sems,
            pltpu.SemaphoreType.DMA,
            pltpu.SemaphoreType.DMA((8,)),
        ],
        compiler_params=pltpu.CompilerParams(collective_id=0, has_side_effects=True),
    )(
        queries, keys, values, hidden, jnp.swapaxes(log_sums, 1, 2), jnp.swapaxes(gates, 1, 2),
        branch_out, cotangent, chosen,
    )
    return pl.pallas_call(
        place_kernel,
        out_shape=tuple(jax.ShapeDtypeStruct(shape, WIDE) for shape in shapes),
        in_specs=[vmem] * len(shapes),
        out_specs=(vmem,) * len(shapes),
    )(*(pltpu.with_memory_space_constraint(result, pltpu.VMEM) for result in results))


def fits(n, tps, hidden, chosen):
    whole = (hidden.shape[1] // n) % 128 == 0 and (hidden.shape[0] // tps) % 16 == 0
    return chosen.shape[0] <= TOPN and n % 2 == 0 and whole


def solution(mesh):

    n, tps = mesh.shape["kv"], mesh.shape["tp"]

    def body(*args):
        return fused(n, tps, *args) if fits(n, tps, args[3], args[8]) else shards(*args)

    return jax.shard_map(
        body,
        mesh=mesh,
        in_specs=(
            P("kv", "tp"),
            P("kv", "tp"),
            P("kv", "tp"),
            P("kv", None),
            P(None, "kv", "tp"),
            P(None, "kv", "tp"),
            P(None, "kv", "tp"),
            P("kv", "tp"),
            P(None, "tp", None),
        ),
        out_specs=(P("kv", "tp"), P("kv", "tp"), P("kv", "tp"), P("kv", "tp")),
        check_vma=False,
    )
```
